32 devices in a mesh: dp: 4 (over y, x), kv: 4 (over z), tp: 2 (over core).
Axes of the slice: x: 2, y: 2, z: 4, core: 2. Of those that a mesh axis runs over, the one named last changes fastest.
Arguments:
- tokens: bfloat16 [16, 24, 2048], P('dp'), may hold values from -6 to 6
- norm_gain: bfloat16 [2048], replicated, may hold values from 0.099609375 to 1.8984375
- w_query: bfloat16 [2048, 1024], P('kv', 'tp'), may hold values from -0.125 to 0.125
- w_key: bfloat16 [2048, 1024], P('kv', 'tp'), may hold values from -0.03125 to 0.03125
- w_value: bfloat16 [2048, 1024], P('kv', 'tp'), may hold values from -0.03125 to 0.03125
- w_forget: bfloat16 [2048, 16], P('kv', 'tp'), may hold values from -0.125 to 0.125
- forget_bias: float32 [16], P('tp'), may hold values from 0 to 4
- head_gain: bfloat16 [1024], P('tp'), may hold values from 0.099609375 to 1.8984375
- w_out: bfloat16 [1024, 2048], P('tp', 'kv'), may hold values from -0.1875 to 0.1875
- cache_keys: bfloat16 [16, 1024, 1024], P('dp', 'kv', 'tp'), may hold values from -480 to 480
- cache_values: bfloat16 [16, 1024, 1024], P('dp', 'kv', 'tp'), may hold values from -1.5 to 1.5
- cache_gates: float32 [16, 16, 1024], P('dp', 'tp', 'kv'), may hold values from -128 to 0, as said below
- lengths: int32 [16], P('dp'), may hold values from 512 to 975
- accepted: int32 [16], P('dp'), may hold values from 0 to 23
- parents: int32 [16, 24], P('dp'), may hold values from -1 to 22, as said below
Outputs:
- mixed: float32 [16, 24, 2048], P('dp', None, ('kv', 'tp'))
- keys_out: bfloat16 [16, 1024, 1024], P('dp', 'kv', 'tp')
- values_out: bfloat16 [16, 1024, 1024], P('dp', 'kv', 'tp')
- gates_out: float32 [16, 16, 1024], P('dp', 'tp', 'kv')
The draws below stay inside these ranges and needn't reach their ends.
Inputs may be any that keep to these rules, and one draw needn't show every extreme that they name: parents[b, 0] = -1 and 0 <= parents[b, j] < j for every later proposal j. `cache_gates`: nonincreasing along the positions of each sequence and head.
All inputs are finite; a program needn't handle non-finite values.
Results may differ from the reference program's by a relative error of at most 0.008.
Values may be sent and summed in bfloat16 or wider, within the bound.
A program may use at most 64 MiB of HBM per device.

```python
import jax
import jax.numpy as jnp
from jax import lax

D = 2048
HEADS = 16
PROP = 24
ATT_WIDTH = 1024
SEQS = 16
LENGTH = 1024


def draw_cache_keys(key, part):
    first_key = jax.random.fold_in(jax.random.fold_in(key, 11), 0)
    array_shape = (SEQS, LENGTH, ATT_WIDTH)
    values = jnp.clip(jax.random.normal(first_key, array_shape, jnp.float32), -6.0, 6.0)
    return values.astype(jnp.bfloat16)


def draw_cache_gates(key, part):
    keys = jax.random.split(jax.random.fold_in(key, 23), 5)
    share = 0.5
    quick = jax.random.uniform(keys[0], (SEQS, HEADS, 1), jnp.float32) < share
    rate_quick = 1.0 / jax.random.uniform(keys[1], (SEQS, HEADS, 1), jnp.float32, 30.0, 100.0)
    rate_slow = jax.random.uniform(keys[2], (SEQS, HEADS, 1), jnp.float32, 0.3, 1.5) / LENGTH
    rates = jnp.where(quick, rate_quick, rate_slow)
    table = jnp.exp(jax.random.uniform(keys[3], (SEQS, HEADS, 16), jnp.float32, -0.7, 0.7))
    block_index = jnp.arange(LENGTH, dtype=jnp.int32) * 16 // LENGTH
    factor = jnp.take(table, block_index, axis=2)
    rough = jax.random.uniform(keys[4], (SEQS, HEADS, LENGTH), jnp.float32, 0.3, 1.7)
    return jnp.cumsum(-rates * factor * rough, axis=2)


def draw_parents(key, part):
    stride = jax.random.randint(jax.random.fold_in(key, 37), (SEQS, PROP), 1, 5)
    indices = jnp.arange(PROP, dtype=jnp.int32)[None, :]
    return jnp.where(indices == 0, -1, jnp.maximum(indices - stride, 0)).astype(jnp.int32)


def set_ends(array, rng, smallest, top_value):
    longest = array.shape.index(max(array.shape))
    spots = []
    for shift in (0, 1):
        where = [jax.random.randint(jax.random.fold_in(rng, axis), (), 0, length) for axis, length in enumerate(array.shape)]
        where[longest] = (where[longest] + shift) % array.shape[longest]
        spots.append(tuple(where))
    return array.at[spots[0]].set(smallest).at[spots[1]].set(top_value)


def levels(stream_key, dims, shards, smallest, largest):
    loudness, own = 1.0, jax.random.fold_in(stream_key, 6)
    for axis_at, blocks in shards:
        heights = jnp.exp(jax.random.uniform(jax.random.fold_in(own, axis_at), (blocks,), jnp.float32, smallest / len(shards), largest / len(shards)))
        loudness = loudness * jnp.repeat(heights, dims[axis_at] // blocks).reshape([-1 if axis == axis_at else 1 for axis in range(len(dims))])
    return loudness


def noise(key, shape, width, bound, cuts=(), kind=jnp.bfloat16):
    result = jax.random.normal(key, shape, jnp.float32) * width
    if len(cuts) > 0:
        result = levels(key, shape, cuts, -0.22, 0.18) * result
    return jnp.clip(result, min=-bound, max=bound).astype(kind)


def setup_inputs(seed: int = 0) -> dict:
    seeds = jax.random.split(jax.random.key(seed), 16)
    tokens = noise(seeds[0], (SEQS, PROP, D), 1.0, 6.0, ((0, 4),))
    norm_gain = jnp.clip(1.0 + 0.18 * jax.random.normal(seeds[1], (D,), jnp.float32), 0.099609375, 1.8984375).astype(jnp.bfloat16)
    w_query = noise(seeds[2], (D, ATT_WIDTH), D ** -0.5, 0.125, ((0, 4), (1, 2)))
    w_key = noise(seeds[3], (D, ATT_WIDTH), (16 * D) ** -0.5, 0.03125, ((0, 4), (1, 2)))
    w_value = noise(seeds[4], (D, ATT_WIDTH), (16 * D) ** -0.5, 0.03125, ((0, 4), (1, 2)))
    w_forget = noise(seeds[5], (D, HEADS), D ** -0.5, 0.125, ((0, 4), (1, 2)))
    forget_bias = jnp.clip(4.0 * jax.random.uniform(seeds[6], (HEADS,), jnp.float32) ** levels(seeds[6], (HEADS,), ((0, 2),), -0.2, 0.2), 0.0, 4.0)
    head_gain = jnp.clip(1.0 + 0.18 * jax.random.normal(seeds[7], (ATT_WIDTH,), jnp.float32), 0.099609375, 1.8984375).astype(jnp.bfloat16)
    w_out = noise(seeds[8], (ATT_WIDTH, D), ATT_WIDTH ** -0.5, 0.1875, ((0, 2), (1, 4)))
    cache_keys = draw_cache_keys(jax.random.fold_in(seeds[15], 71), 0)
    cache_values = noise(seeds[10], (SEQS, LENGTH, ATT_WIDTH), 0.25, 1.5, ((0, 4), (1, 4), (2, 2)))
    cache_gates = draw_cache_gates(jax.random.fold_in(seeds[15], 71), 0)
    lengths = set_ends(jax.random.randint(seeds[12], (SEQS,), LENGTH // 2, LENGTH - 2 * PROP), jax.random.fold_in(seeds[12], 1), LENGTH // 2, (LENGTH - 2 * PROP) - 1).astype(jnp.int32)
    accepted = set_ends(jax.random.randint(seeds[13], (SEQS,), 0, PROP), jax.random.fold_in(seeds[13], 1), 0, PROP - 1).astype(jnp.int32)
    parents = draw_parents(jax.random.fold_in(seeds[15], 71), 0)
    return {"tokens": tokens, "norm_gain": norm_gain, "w_query": w_query, "w_key": w_key, "w_value": w_value, "w_forget": w_forget, "forget_bias": forget_bias, "head_gain": head_gain, "w_out": w_out, "cache_keys": cache_keys, "cache_values": cache_values, "cache_gates": cache_gates, "lengths": lengths, "accepted": accepted, "parents": parents}


NEG_LARGE = -1e+30
EPSILON = 1e-06

def ancestry(parents):
    prop_count = parents.shape[1]
    indices = jnp.arange(prop_count, dtype=jnp.int32)
    linked = (parents[:, :, None] == indices[None, None, :]).astype(jnp.float32)
    linked = linked + (indices[:, None] == indices[None, :]).astype(jnp.float32)[None]
    for repeat in range(prop_count.bit_length()):
        linked = jnp.minimum(jnp.einsum('bij,bjk->bik', linked, linked, precision=lax.Precision.HIGHEST), 1.0)
    return linked

def reference(tokens, norm_gain, w_query, w_key, w_value, w_forget, forget_bias, head_gain, w_out, cache_keys, cache_values, cache_gates, lengths, accepted, parents):
    seq_count, prop_count, model_width = tokens.shape
    head_count = cache_gates.shape[1]
    full_length = cache_gates.shape[2]
    head_size = cache_keys.shape[2] // head_count
    flat_rows = tokens.reshape(seq_count * prop_count, model_width).astype(jnp.float32)
    normed = (flat_rows * lax.rsqrt(lax.optimization_barrier(jnp.mean(flat_rows * flat_rows, axis=1, keepdims=True)) + EPSILON) * norm_gain.astype(jnp.float32)).astype(jnp.bfloat16)
    query = jnp.dot(normed, w_query, preferred_element_type=jnp.float32).astype(jnp.bfloat16)
    fresh_keys = jnp.dot(normed, w_key, preferred_element_type=jnp.float32).astype(jnp.bfloat16)
    fresh_values = jnp.dot(normed, w_value, preferred_element_type=jnp.float32).astype(jnp.bfloat16)
    query = query.reshape(seq_count, prop_count, head_count, head_size)
    fresh_keys = fresh_keys.reshape(seq_count, prop_count, head_count, head_size)
    fresh_values = fresh_values.reshape(seq_count, prop_count, head_count, head_size)
    log_gate = jax.nn.log_sigmoid(jnp.dot(normed, w_forget, preferred_element_type=jnp.float32) + forget_bias.astype(jnp.float32)).reshape(seq_count, prop_count, head_count)
    valid_len = (lengths + accepted).astype(jnp.int32)
    link = ancestry(parents)
    climb = jnp.einsum('bia,bah->bih', link, log_gate, precision=lax.Precision.HIGHEST)
    positions = jnp.arange(full_length, dtype=jnp.int32)
    scale = head_size ** (-0.5)
    gain_rows = head_gain.astype(jnp.float32).reshape(head_count, head_size)
    zero_index = jnp.zeros((), jnp.int32)

    def one_sequence(entry):
        q_rows, new_keys, new_values, climb_row, link_row, stored_keys, stored_values, stored_gates, valid_row = entry
        last_gate = lax.dynamic_slice_in_dim(stored_gates, valid_row - 1, 1, 1)[:, 0]
        key_rows = stored_keys.reshape(full_length, head_count, head_size).astype(jnp.float32)
        value_rows = stored_values.reshape(full_length, head_count, head_size).astype(jnp.float32)
        q_float = q_rows.astype(jnp.float32)
        far_scores = jnp.einsum('phd,chd->phc', q_float, key_rows) * scale
        far_scores = far_scores + (last_gate[None, :] + climb_row)[:, :, None] - stored_gates[None]
        far_mask = (positions < valid_row)[None, None, :]
        far_scores = jnp.where(far_mask, far_scores, NEG_LARGE)
        near_scores = jnp.einsum('phd,ahd->pha', q_float, new_keys.astype(jnp.float32)) * scale
        near_scores = near_scores + climb_row[:, :, None] - jnp.transpose(climb_row)[None]
        near_mask = (link_row > 0.5)[:, None, :]
        near_scores = jnp.where(near_mask, near_scores, NEG_LARGE)
        highest = jnp.maximum(lax.optimization_barrier(jnp.max(far_scores, axis=2)), lax.optimization_barrier(jnp.max(near_scores, axis=2)))
        far_weights = jnp.where(far_mask, jnp.exp(far_scores - highest[:, :, None]), 0.0)
        near_weights = jnp.where(near_mask, jnp.exp(near_scores - highest[:, :, None]), 0.0)
        normalizer = lax.optimization_barrier(jnp.sum(far_weights, axis=2)) + lax.optimization_barrier(jnp.sum(near_weights, axis=2))
        far_rounded = lax.optimization_barrier(far_weights.astype(jnp.bfloat16)).astype(jnp.float32)
        near_rounded = lax.optimization_barrier(near_weights.astype(jnp.bfloat16)).astype(jnp.float32)
        attended = jnp.einsum('phc,chd->phd', far_rounded, value_rows)
        attended = attended + jnp.einsum('pha,ahd->phd', near_rounded, new_values.astype(jnp.float32))
        attended = attended / normalizer[:, :, None]
        heads_out = attended * lax.rsqrt(lax.optimization_barrier(jnp.mean(attended * attended, axis=2, keepdims=True)) + EPSILON) * gain_rows[None]
        keys_out = lax.dynamic_update_slice(stored_keys, new_keys.reshape(prop_count, head_count * head_size), (valid_row, zero_index))
        values_out = lax.dynamic_update_slice(stored_values, new_values.reshape(prop_count, head_count * head_size), (valid_row, zero_index))
        gates_out = lax.dynamic_update_slice(stored_gates, last_gate[:, None] + jnp.transpose(climb_row), (zero_index, valid_row))
        return (heads_out.astype(jnp.bfloat16).reshape(prop_count, head_count * head_size), keys_out, values_out, gates_out)
    heads_all, keys_out, values_out, gates_out = lax.map(one_sequence, (query, fresh_keys, fresh_values, climb, link, cache_keys, cache_values, cache_gates, valid_len))
    flat_heads = heads_all.reshape(seq_count * prop_count, head_count * head_size)
    mixed = jnp.dot(flat_heads, w_out, preferred_element_type=jnp.float32).reshape(seq_count, prop_count, model_width)
    return (mixed, keys_out, values_out, gates_out)
```

```python
import functools

import jax
import jax.numpy as jnp
from jax import lax
from jax.experimental import pallas as pl
from jax.experimental.pallas import tpu as pltpu
from jax.sharding import PartitionSpec as P

NEG_LARGE = -1e30
EPSILON = 1e-06


def joined_2(value, axis, join):
    pieces = jax.tree.map(lambda part: lax.all_gather(part, axis), value)
    head = jax.tree.map(lambda part: part[0], pieces)
    tail = jax.tree.map(lambda part: part[1:], pieces)
    total, _ = lax.scan(lambda total, piece: (join(total, piece), None), head, tail)
    return total


def ancestry(parents):
    prop_count = parents.shape[1]
    indices = jnp.arange(prop_count, dtype=jnp.int32)
    linked = (parents[:, :, None] == indices[None, None, :]).astype(jnp.float32)
    linked = linked + (indices[:, None] == indices[None, :]).astype(jnp.float32)[None]
    for repeat in range(prop_count.bit_length()):
        linked = jnp.minimum(
            jnp.einsum("bij,bjk->bik", linked, linked, precision=lax.Precision.HIGHEST), 1.0
        )
    return linked


def merge_pair(first_part, second_part):
    highest = jnp.maximum(first_part[0], second_part[0])
    scale_first = jnp.exp(first_part[0] - highest)
    scale_second = jnp.exp(second_part[0] - highest)
    seq_count, prop_count, head_count = highest.shape
    outer_first = (
        first_part[2].reshape(seq_count, prop_count, head_count, -1) * scale_first[..., None]
    )
    outer_second = (
        second_part[2].reshape(seq_count, prop_count, head_count, -1) * scale_second[..., None]
    )
    joined = (outer_first + outer_second).reshape(seq_count, prop_count, -1)
    return (highest, first_part[1] * scale_first + second_part[1] * scale_second, joined)


def local(
    tokens,
    norm_gain,
    w_query,
    w_key,
    w_value,
    w_forget,
    forget_bias,
    head_gain,
    w_out,
    cache_keys,
    cache_values,
    cache_gates,
    lengths,
    accepted,
    parents,
):
    seq_count, prop_count, model_width = tokens.shape
    span_rows = cache_keys.shape[1]
    head_count = cache_gates.shape[1]
    head_size = cache_keys.shape[2] // head_count
    scale = head_size ** (-0.5)
    start_pos = lax.axis_index("kv") * span_rows
    positions = start_pos + jnp.arange(span_rows, dtype=jnp.int32)
    valid_len = lengths + accepted
    flat_rows = tokens.reshape(seq_count * prop_count, model_width).astype(jnp.float32)
    normed = (
        flat_rows
        * lax.rsqrt(jnp.mean(flat_rows * flat_rows, axis=1, keepdims=True) + EPSILON)
        * norm_gain.astype(jnp.float32)
    ).astype(jnp.bfloat16)
    picked = (positions[None, :] == (valid_len - 1)[:, None]).astype(jnp.float32)
    last_part = jnp.sum(cache_gates * picked[:, None, :], axis=2)
    row_count = w_query.shape[0]
    own_columns = lax.dynamic_slice_in_dim(normed, lax.axis_index("kv") * row_count, row_count, 1)
    query_part = jnp.dot(own_columns, w_query, preferred_element_type=jnp.float32)
    key_part = jnp.dot(own_columns, w_key, preferred_element_type=jnp.float32)
    value_part = jnp.dot(own_columns, w_value, preferred_element_type=jnp.float32)
    gate_part = jnp.dot(own_columns, w_forget, preferred_element_type=jnp.float32)
    query, fresh_keys, fresh_values, gate_pre, last_gate = lax.psum(
        (query_part, key_part, value_part, gate_part, last_part), "kv"
    )
    query = query.astype(jnp.bfloat16).reshape(seq_count, prop_count, head_count, head_size)
    fresh_keys = fresh_keys.astype(jnp.bfloat16).reshape(
        seq_count, prop_count, head_count, head_size
    )
    fresh_values = fresh_values.astype(jnp.bfloat16).reshape(
        seq_count, prop_count, head_count, head_size
    )
    log_gate = jax.nn.log_sigmoid(gate_pre + forget_bias).reshape(seq_count, prop_count, head_count)
    link = ancestry(parents)
    climb = jnp.einsum("bia,bah->bih", link, log_gate, precision=lax.Precision.HIGHEST)
    stored_keys = cache_keys.reshape(seq_count, span_rows, head_count, head_size)
    stored_values = cache_values.reshape(seq_count, span_rows, head_count, head_size)
    scores = (
        jnp.einsum("bphd,bchd->bphc", query, stored_keys, preferred_element_type=jnp.float32)
        * scale
    )
    scores = scores + (last_gate[:, None, :] + climb)[..., None] - cache_gates[:, None]
    seen = (positions[None, :] < valid_len[:, None])[:, None, None, :]
    highest = jnp.max(jnp.where(seen, scores, NEG_LARGE), axis=3)
    weights = jnp.where(seen, jnp.exp(scores - highest[..., None]), 0.0)
    normalizer = jnp.sum(weights, axis=3)
    weighted = jnp.einsum(
        "bphc,bchd->bphd",
        weights.astype(jnp.bfloat16),
        stored_values,
        preferred_element_type=jnp.float32,
    )
    highest, normalizer, weighted = joined_2(
        (highest, normalizer, weighted.reshape(seq_count, prop_count, head_count * head_size)),
        "kv",
        merge_pair,
    )
    near_scores = (
        jnp.einsum("bphd,bahd->bpha", query, fresh_keys, preferred_element_type=jnp.float32) * scale
    )
    near_scores = near_scores + climb[..., None] - jnp.transpose(climb, (0, 2, 1))[:, None]
    linked = (link > 0.5)[:, :, None, :]
    near_high = jnp.max(jnp.where(linked, near_scores, NEG_LARGE), axis=3)
    overall = jnp.maximum(highest, near_high)
    carried = jnp.exp(highest - overall)
    near_weights = jnp.where(linked, jnp.exp(near_scores - overall[..., None]), 0.0)
    normalizer = normalizer * carried + jnp.sum(near_weights, axis=3)
    attended = weighted.reshape(seq_count, prop_count, head_count, head_size) * carried[..., None]
    attended = attended + jnp.einsum(
        "bpha,bahd->bphd",
        near_weights.astype(jnp.bfloat16),
        fresh_values,
        preferred_element_type=jnp.float32,
    )
    attended = attended / normalizer[..., None]
    gain_rows = head_gain.astype(jnp.float32).reshape(head_count, head_size)
    heads_out = (
        (
            attended
            * lax.rsqrt(jnp.mean(attended * attended, axis=3, keepdims=True) + EPSILON)
            * gain_rows
        )
        .astype(jnp.bfloat16)
        .reshape(seq_count * prop_count, head_count * head_size)
    )
    partial_sum = jnp.dot(heads_out, w_out, preferred_element_type=jnp.float32)
    summed = lax.psum_scatter(partial_sum, "tp", scatter_dimension=1, tiled=True)
    mixed = summed.reshape(seq_count, prop_count, -1)
    offsets = positions[None, :, None] - valid_len[:, None, None]
    placed = offsets == jnp.arange(prop_count, dtype=jnp.int32)[None, None, :]
    landed = jnp.any(placed, axis=2)
    placed_low = placed.astype(jnp.bfloat16)
    written_keys = jnp.einsum(
        "bcj,bjx->bcx",
        placed_low,
        fresh_keys.reshape(seq_count, prop_count, -1),
        preferred_element_type=jnp.float32,
    ).astype(jnp.bfloat16)
    written_values = jnp.einsum(
        "bcj,bjx->bcx",
        placed_low,
        fresh_values.reshape(seq_count, prop_count, -1),
        preferred_element_type=jnp.float32,
    ).astype(jnp.bfloat16)
    keys_out = jnp.where(landed[..., None], written_keys, cache_keys)
    values_out = jnp.where(landed[..., None], written_values, cache_values)
    new_gates = last_gate[:, :, None] + jnp.transpose(climb, (0, 2, 1))
    written_gates = jnp.einsum(
        "bcj,bhj->bhc", placed.astype(jnp.float32), new_gates, precision=lax.Precision.HIGHEST
    )
    gates_out = jnp.where(landed[:, None, :], written_gates, cache_gates)
    return (mixed, keys_out, values_out, gates_out)


HIGHEST = lax.Precision.HIGHEST
MESH = pl.DeviceIdType.MESH
LANES = 128


def dot_rows(left, right, precision=None):
    return lax.dot_general(
        left,
        right,
        (((1,), (1,)), ((), ())),
        precision=precision,
        preferred_element_type=jnp.float32,
    )


def dot_plain(left, right, precision=None):
    return jnp.dot(left, right, precision=precision, preferred_element_type=jnp.float32)


def exchange_kernel(
    kv_count,
    head_count,
    lengths_ref,
    accepted_ref,
    tokens_hbm,
    gain_hbm,
    wq_hbm,
    wk_hbm,
    wv_hbm,
    wf_hbm,
    bias_hbm,
    head_gain_hbm,
    wo_hbm,
    keys_hbm,
    values_hbm,
    gates_hbm,
    parents_hbm,
    mixed_out,
    fresh_out,
    fresh_gates_out,
    tokens_ref,
    gain_ref,
    wq_ref,
    wk_ref,
    wv_ref,
    wf_ref,
    bias_ref,
    head_gain_ref,
    wo_ref,
    keys_ref,
    values_ref,
    gates_ref,
    parents_ref,
    q_send,
    q_recv,
    q_all,
    kv_send,
    kv_recv,
    kv_all,
    g_send,
    g_recv,
    g_all,
    w_send,
    w_recv,
    st_send,
    st_recv,
    h_all,
    o_send,
    o_recv,
    load_sem,
    send_sem,
    recv_sem,
    pair_sem,
):
    dp, me, tp = lax.axis_index("dp"), lax.axis_index("kv"), lax.axis_index("tp")
    seq_count, prop, _ = tokens_ref.shape
    depth, width = wq_ref.shape
    span = keys_ref.shape[1]
    head_size = width // head_count
    scale = head_size ** (-0.5)
    rows_all = head_count * prop
    half = wo_ref.shape[1] // 2
    offsets = range(1, kv_count)

    sources = (
        (tokens_hbm, tokens_ref),
        (gain_hbm, gain_ref),
        (wq_hbm, wq_ref),
        (wk_hbm, wk_ref),
        (wv_hbm, wv_ref),
        (wf_hbm, wf_ref),
        (gates_hbm, gates_ref),
        (keys_hbm, keys_ref),
        (values_hbm, values_ref),
        (parents_hbm, parents_ref),
        (bias_hbm, bias_ref),
        (head_gain_hbm, head_gain_ref),
        (wo_hbm, wo_ref),
    )
    loads = {}
    for at, (source, target) in enumerate(sources):
        copy = pltpu.make_async_copy(source, target, load_sem.at[at])
        copy.start()
        loads[id(target)] = copy

    def loaded(*refs):
        for ref in refs:
            loads[id(ref)].wait()

    barrier = pltpu.get_barrier_semaphore()
    for offset in offsets:
        pl.semaphore_signal(
            barrier,
            inc=1,
            device_id=(dp, lax.rem(me + offset, kv_count), tp),
            device_id_type=MESH,
        )
    pl.semaphore_signal(barrier, inc=1, device_id=(dp, me, 1 - tp), device_id_type=MESH)

    started = []

    def send(kind, offset, source, target):
        copy = pltpu.make_async_remote_copy(
            src_ref=source,
            dst_ref=target,
            send_sem=send_sem.at[kind, offset],
            recv_sem=recv_sem.at[kind, offset],
            device_id=(dp, lax.rem(me + offset, kv_count), tp),
            device_id_type=MESH,
        )
        copy.start()
        started.append(copy)
        return copy

    loaded(tokens_ref, gain_ref)
    flat = jnp.concatenate([tokens_ref[s].astype(jnp.float32) for s in range(seq_count)], 0)
    inverse = lax.rsqrt(jnp.mean(flat * flat, axis=1, keepdims=True) + EPSILON)
    start = pl.multiple_of(me * depth, depth)
    own = jnp.concatenate(
        [tokens_ref[s, :, pl.ds(start, depth)].astype(jnp.float32) for s in range(seq_count)], 0
    )
    own_gain = gain_ref[:, pl.ds(start, depth)].astype(jnp.float32)
    normed = (own * inverse * own_gain).astype(jnp.bfloat16)
    loaded(wq_ref)
    q_part = dot_plain(normed, wq_ref[...])
    for s in range(seq_count):
        q_send[s] = q_part[s * prop : (s + 1) * prop]
    pl.semaphore_wait(barrier, kv_count)
    q_copies = [
        send(0, offset, q_send.at[lax.rem(me + offset, kv_count)], q_recv.at[offset])
        for offset in offsets
    ]

    loaded(wk_ref, wv_ref, wf_ref, gates_ref)
    k_part = dot_plain(normed, wk_ref[...])
    v_part = dot_plain(normed, wv_ref[...])
    f_part = dot_plain(normed, wf_ref[...])
    lane_pos = lax.broadcasted_iota(jnp.int32, (head_count, span), 1) + me * span
    for s in range(seq_count):
        rows = slice(s * prop, (s + 1) * prop)
        kv_send[s, 0] = k_part[rows].astype(jnp.bfloat16)
        kv_send[s, 1] = v_part[rows].astype(jnp.bfloat16)
        valid = lengths_ref[s] + accepted_ref[s]
        picked = jnp.where(lane_pos == valid - 1, gates_ref[s], 0.0)
        last = jnp.sum(picked, axis=1, keepdims=True)
        g_send[s, :prop, :] = jnp.zeros((prop, LANES), jnp.float32)
        g_send[s, :prop, :head_count] = f_part[rows]
        g_send[s, prop:, :] = jnp.broadcast_to(last, (head_count, LANES))

    loaded(parents_ref)
    parent_row = parents_ref[pl.ds(me, 1), :]
    up = lax.broadcasted_iota(jnp.int32, (prop, prop), 0)
    down = lax.broadcasted_iota(jnp.int32, (prop, prop), 1)
    eye = (up == down).astype(jnp.bfloat16)
    linked = jnp.where((up == parent_row) | (up == down), 1.0, 0.0)
    for repeat in range(prop.bit_length()):
        low = linked.astype(jnp.bfloat16)
        linked = jnp.minimum(dot_plain(low, low), 1.0)
    link = dot_rows(eye, linked.astype(jnp.bfloat16))

    total = q_send[me]
    for copy, offset in zip(q_copies, offsets):
        copy.wait_recv()
        total = total + q_recv[offset]
    q_all[me] = total.astype(jnp.bfloat16)
    qa_copies = {offset: send(1, offset, q_all.at[me], q_all.at[me]) for offset in offsets}
    kv_copies = []
    for offset in offsets:
        there = lax.rem(me + offset, kv_count)
        kv_copies.append(send(2, offset, kv_send.at[there], kv_recv.at[offset]))
        kv_copies.append(send(3, offset, g_send.at[there], g_recv.at[offset]))

    shape = (head_count, prop, width)
    head_mask = (
        lax.broadcasted_iota(jnp.int32, shape, 2) // head_size
        == lax.broadcasted_iota(jnp.int32, shape, 0)
    )
    small = (head_count, prop, LANES)
    small_lane = lax.broadcasted_iota(jnp.int32, small, 2)
    small_head = lax.broadcasted_iota(jnp.int32, small, 0)

    def spread(query):
        wide = jnp.broadcast_to(query.astype(jnp.float32)[None], shape)
        return jnp.where(head_mask, wide, 0.0).reshape(rows_all, width).astype(jnp.bfloat16)

    def fold(wide):
        return jnp.sum(jnp.where(head_mask, wide.reshape(shape), 0.0), axis=0)

    def expand(column):
        return fold(jnp.broadcast_to(column, (rows_all, width)))

    def column_of(compact, first_lane):
        wide = jnp.broadcast_to(compact[None], small)
        taken = jnp.where(small_lane == small_head + first_lane, wide, 0.0)
        return jnp.sum(taken.reshape(rows_all, LANES), axis=1, keepdims=True)

    score_pos = lax.broadcasted_iota(jnp.int32, (rows_all, span), 1) + me * span

    def attend(s):
        valid = lengths_ref[s] + accepted_ref[s]
        scores = dot_rows(spread(q_all[s]), keys_ref[s]) * scale
        gates = jnp.broadcast_to(gates_ref[s][:, None, :], (head_count, prop, span))
        scores = scores - gates.reshape(rows_all, span)
        seen = score_pos < valid
        highest = jnp.max(jnp.where(seen, scores, NEG_LARGE), axis=1, keepdims=True)
        weights = jnp.where(seen, jnp.exp(scores - highest), 0.0)
        normalizer = jnp.sum(weights, axis=1, keepdims=True)
        w_send[s] = fold(dot_plain(weights.astype(jnp.bfloat16), values_ref[s])).astype(
            jnp.bfloat16
        )
        both = jnp.where(
            small_lane == small_head,
            highest.reshape(head_count, prop, 1),
            jnp.where(
                small_lane == small_head + head_count,
                normalizer.reshape(head_count, prop, 1),
                0.0,
            ),
        )
        st_send[s] = jnp.sum(both, axis=0)

    loaded(keys_ref, values_ref)
    attend(me)
    w_copies = {}
    for offset in offsets:
        qa_copies[offset].wait_recv()
        back = kv_count - offset
        there = lax.rem(me + back, kv_count)
        attend(there)
        w_copies[back] = (
            send(4, back, w_send.at[there], w_recv.at[back]),
            send(5, back, st_send.at[there], st_recv.at[back]),
        )

    for copy in kv_copies:
        copy.wait_recv()
    fresh_k = kv_send[me, 0].astype(jnp.float32)
    fresh_v = kv_send[me, 1].astype(jnp.float32)
    gate_sum = g_send[me]
    for offset in offsets:
        fresh_k = fresh_k + kv_recv[offset, 0].astype(jnp.float32)
        fresh_v = fresh_v + kv_recv[offset, 1].astype(jnp.float32)
        gate_sum = gate_sum + g_recv[offset]
    fresh_k = fresh_k.astype(jnp.bfloat16)
    fresh_v = fresh_v.astype(jnp.bfloat16)
    kv_all[me, 0] = fresh_k
    kv_all[me, 1] = fresh_v
    loaded(bias_ref)
    gate_pre = gate_sum[:prop, :head_count] + bias_ref[...]
    log_gate = -(jnp.maximum(-gate_pre, 0.0) + jnp.log1p(jnp.exp(-jnp.abs(gate_pre))))
    climb = dot_plain(link, log_gate, HIGHEST)
    chosen = (
        lax.broadcasted_iota(jnp.int32, (head_count, head_count), 0)
        == lax.broadcasted_iota(jnp.int32, (head_count, head_count), 1)
    ).astype(jnp.float32)
    climb_rows = dot_rows(chosen, climb, HIGHEST)
    last_wide = gate_sum[prop:]
    g_all[me] = jnp.zeros((head_count, LANES), jnp.float32)
    g_all[me, :, :prop] = last_wide[:, :prop] + climb_rows

    wide_climb = jnp.broadcast_to(climb[None], (head_count, prop, head_count))
    climb_lane = lax.broadcasted_iota(jnp.int32, (head_count, prop, head_count), 2)
    climb_head = lax.broadcasted_iota(jnp.int32, (head_count, prop, head_count), 0)
    climb_col = jnp.sum(
        jnp.where(climb_lane == climb_head, wide_climb, 0.0).reshape(rows_all, head_count),
        axis=1,
        keepdims=True,
    )
    near_shape = (head_count, prop, prop)
    near = dot_rows(spread(q_all[me]), fresh_k) * scale + climb_col
    near = near - jnp.broadcast_to(climb_rows[:, None, :], near_shape).reshape(rows_all, prop)
    near_link = jnp.broadcast_to(link[None], near_shape).reshape(rows_all, prop) > 0.5
    near_high = jnp.max(jnp.where(near_link, near, NEG_LARGE), axis=1, keepdims=True)
    near_weights = jnp.where(near_link, jnp.exp(near - near_high), 0.0)
    near_sum = jnp.sum(near_weights, axis=1, keepdims=True)
    near_wide = dot_plain(near_weights.astype(jnp.bfloat16), fresh_v)
    last_col = jnp.broadcast_to(
        last_wide[:, None, :1], (head_count, prop, 1)
    ).reshape(rows_all, 1)
    shift = last_col + climb_col

    loaded(head_gain_ref)
    for pair in w_copies.values():
        for copy in pair:
            copy.wait_recv()
    stats = [st_send[me]] + [st_recv[offset] for offset in offsets]
    parts = [w_send[me]] + [w_recv[offset] for offset in offsets]
    highs = [column_of(stat, 0) + shift for stat in stats]
    sums = [column_of(stat, head_count) for stat in stats]
    overall = near_high
    for high in highs:
        overall = jnp.maximum(overall, high)
    near_factor = jnp.exp(near_high - overall)
    factors = [jnp.exp(high - overall) for high in highs]
    normalizer = near_sum * near_factor
    for factor, part in zip(factors, sums):
        normalizer = normalizer + factor * part
    attended = fold(near_wide * (near_factor / normalizer))
    for factor, part in zip(factors, parts):
        attended = attended + expand(factor / normalizer) * part.astype(jnp.float32)
    squares = jnp.where(head_mask, jnp.broadcast_to((attended * attended)[None], shape), 0.0)
    square_col = jnp.sum(squares.reshape(rows_all, width), axis=1, keepdims=True)
    rooted = lax.rsqrt(square_col * (1.0 / head_size) + EPSILON)
    head_out = attended * expand(rooted) * head_gain_ref[...].astype(jnp.float32)
    h_all[me] = head_out.astype(jnp.bfloat16)
    h_copies = [send(6, offset, h_all.at[me], h_all.at[me]) for offset in offsets]
    fresh_copies = []
    for offset in offsets:
        fresh_copies.append(send(7, offset, kv_all.at[me], kv_all.at[me]))
        fresh_copies.append(send(8, offset, g_all.at[me], g_all.at[me]))

    loaded(wo_ref)
    for copy in h_copies:
        copy.wait_recv()
    heads = jnp.concatenate(
        [h_all[s].astype(jnp.float32) for s in range(seq_count)], 0
    ).astype(jnp.bfloat16)
    there = pl.multiple_of((1 - tp) * half, half)
    here = pl.multiple_of(tp * half, half)
    o_send[...] = dot_plain(heads, wo_ref[:, pl.ds(there, half)])
    pair = pltpu.make_async_remote_copy(
        src_ref=o_send,
        dst_ref=o_recv,
        send_sem=pair_sem.at[0],
        recv_sem=pair_sem.at[1],
        device_id=(dp, me, 1 - tp),
        device_id_type=MESH,
    )
    pair.start()
    own_sum = dot_plain(heads, wo_ref[:, pl.ds(here, half)])
    pair.wait()
    own_sum = own_sum + o_recv[...]
    for s in range(seq_count):
        mixed_out[s] = own_sum[s * prop : (s + 1) * prop]
    for copy in fresh_copies:
        copy.wait_recv()
    fresh_out[...] = kv_all[...]
    fresh_gates_out[...] = g_all[...]
    for copy in started:
        copy.wait_send()


def write_kernel(
    lengths_ref,
    accepted_ref,
    mixed_ref,
    fresh_ref,
    fresh_gates_ref,
    keys_ref,
    values_ref,
    gates_ref,
    mixed_out,
    keys_out,
    values_out,
    gates_out,
):
    seq = pl.program_id(0)
    span = keys_ref.shape[1]
    prop = fresh_ref.shape[2]
    head_count = gates_ref.shape[1]
    valid = lengths_ref[seq] + accepted_ref[seq]
    first = lax.axis_index("kv") * span - valid
    mixed_out[...] = mixed_ref[...]
    down = lax.broadcasted_iota(jnp.int32, (span, prop), 0) + first
    placed = (down == lax.broadcasted_iota(jnp.int32, (span, prop), 1)).astype(jnp.bfloat16)
    row = lax.broadcasted_iota(jnp.int32, (span, keys_ref.shape[2]), 0) + first
    landed = (row >= 0) & (row < prop)
    for at, (source, target) in enumerate(((keys_ref, keys_out), (values_ref, values_out))):
        written = dot_plain(placed, fresh_ref[0, at])
        target[0] = jnp.where(landed, written, source[0].astype(jnp.float32)).astype(jnp.bfloat16)
    over = lax.broadcasted_iota(jnp.int32, (prop, span), 1) + first
    spot = (over == lax.broadcasted_iota(jnp.int32, (prop, span), 0)).astype(jnp.float32)
    new_gates = dot_plain(fresh_gates_ref[0][:, :prop], spot, HIGHEST)
    lane = lax.broadcasted_iota(jnp.int32, (head_count, span), 1) + first
    gates_out[0] = jnp.where((lane >= 0) & (lane < prop), new_gates, gates_ref[0])


def fused(
    kv_count,
    tokens,
    norm_gain,
    w_query,
    w_key,
    w_value,
    w_forget,
    forget_bias,
    head_gain,
    w_out,
    cache_keys,
    cache_values,
    cache_gates,
    lengths,
    accepted,
    parents,
):
    seq_count, prop, _ = tokens.shape
    span, width = cache_keys.shape[1:]
    head_count = cache_gates.shape[1]
    half = w_out.shape[1] // 2
    gain = norm_gain.reshape(1, -1)
    bias = forget_bias.reshape(1, -1)
    head_gain = head_gain.reshape(1, -1)
    low, high = jnp.bfloat16, jnp.float32
    large = (
        tokens, gain, w_query, w_key, w_value, w_forget, bias, head_gain, w_out,
        cache_keys, cache_values, cache_gates, parents,
    )
    vmem = pltpu.VMEM
    scratch = [vmem(value.shape, value.dtype) for value in large]
    block = (seq_count, prop, width)
    pair = (seq_count, 2, prop, width)
    scratch += [
        vmem(block, high),
        vmem(block, high),
        vmem(block, low),
        vmem(pair, low),
        vmem(pair, low),
        vmem(pair, low),
        vmem((seq_count, prop + head_count, LANES), high),
        vmem((seq_count, prop + head_count, LANES), high),
        vmem((seq_count, head_count, LANES), high),
        vmem(block, low),
        vmem(block, low),
        vmem((seq_count, prop, LANES), high),
        vmem((seq_count, prop, LANES), high),
        vmem(block, low),
        vmem((seq_count * prop, half), high),
        vmem((seq_count * prop, half), high),
        pltpu.SemaphoreType.DMA((len(large),)),
        pltpu.SemaphoreType.DMA((9, kv_count)),
        pltpu.SemaphoreType.DMA((9, kv_count)),
        pltpu.SemaphoreType.DMA((2,)),
    ]
    smem = pl.BlockSpec(memory_space=pltpu.SMEM)
    mixed, fresh, fresh_gates = pl.pallas_call(
        functools.partial(exchange_kernel, kv_count, head_count),
        out_shape=(
            jax.ShapeDtypeStruct((seq_count, prop, half), high),
            jax.ShapeDtypeStruct(pair, low),
            jax.ShapeDtypeStruct((seq_count, head_count, LANES), high),
        ),
        in_specs=[smem, smem] + [pl.BlockSpec(memory_space=pl.ANY)] * len(large),
        out_specs=(pl.BlockSpec(memory_space=pltpu.VMEM),) * 3,
        scratch_shapes=scratch,
        compiler_params=pltpu.CompilerParams(
            collective_id=0, has_side_effects=True, vmem_limit_bytes=32 * 1024 * 1024
        ),
        name="exchange",
    )(lengths, accepted, *large)

    def per_seq(*tail):
        return pl.BlockSpec((1, *tail), lambda s: (s,) + (0,) * len(tail))

    outs = (per_seq(prop, half), per_seq(span, width), per_seq(span, width), per_seq(head_count, span))
    return pl.pallas_call(
        write_kernel,
        grid=(seq_count,),
        out_shape=(
            jax.ShapeDtypeStruct(mixed.shape, high),
            jax.ShapeDtypeStruct(cache_keys.shape, low),
            jax.ShapeDtypeStruct(cache_values.shape, low),
            jax.ShapeDtypeStruct(cache_gates.shape, high),
        ),
        in_specs=[
            smem,
            smem,
            outs[0],
            per_seq(2, prop, width),
            per_seq(head_count, LANES),
            outs[1],
            outs[2],
            outs[3],
        ],
        out_specs=outs,
        name="write",
    )(lengths, accepted, mixed, fresh, fresh_gates, cache_keys, cache_values, cache_gates)


def device_step(kv_count, tp_count, tokens, *rest):
    seq_count, prop, _ = tokens.shape
    head_count = rest[10].shape[1]
    fits = seq_count == kv_count and tp_count == 2 and prop % 8 == 0 and prop <= LANES
    if fits and kv_count > 1 and head_count % 8 == 0 and 2 * head_count <= LANES:
        return fused(kv_count, tokens, *rest)
    return local(tokens, *rest)


def solution(mesh):
    placed = (
        P("dp", None, None),
        P(),
        P("kv", "tp"),
        P("kv", "tp"),
        P("kv", "tp"),
        P("kv", "tp"),
        P("tp"),
        P("tp"),
        P("tp", "kv"),
        P("dp", "kv", "tp"),
        P("dp", "kv", "tp"),
        P("dp", "tp", "kv"),
        P("dp"),
        P("dp"),
        P("dp", None),
    )
    return jax.shard_map(
        functools.partial(device_step, mesh.shape["kv"], mesh.shape["tp"]),
        mesh=mesh,
        in_specs=placed,
        out_specs=(
            P("dp", None, ("kv", "tp")),
            P("dp", "kv", "tp"),
            P("dp", "kv", "tp"),
            P("dp", "tp", "kv"),
        ),
        check_vma=False,
    )
```

```python
import functools

import jax
import jax.numpy as jnp
from jax import lax
from jax.experimental import pallas as pl
from jax.experimental.pallas import tpu as pltpu
from jax.sharding import PartitionSpec as P

NEG_LARGE = -1e30
EPSILON = 1e-06


def joined_2(value, axis, join):
    pieces = jax.tree.map(lambda part: lax.all_gather(part, axis), value)
    head = jax.tree.map(lambda part: part[0], pieces)
    tail = jax.tree.map(lambda part: part[1:], pieces)
    total, _ = lax.scan(lambda total, piece: (join(total, piece), None), head, tail)
    return total


def ancestry(parents):
    prop_count = parents.shape[1]
    indices = jnp.arange(prop_count, dtype=jnp.int32)
    linked = (parents[:, :, None] == indices[None, None, :]).astype(jnp.float32)
    linked = linked + (indices[:, None] == indices[None, :]).astype(jnp.float32)[None]
    for repeat in range(prop_count.bit_length()):
        linked = jnp.minimum(
            jnp.einsum("bij,bjk->bik", linked, linked, precision=lax.Precision.HIGHEST), 1.0
        )
    return linked


def merge_pair(first_part, second_part):
    highest = jnp.maximum(first_part[0], second_part[0])
    scale_first = jnp.exp(first_part[0] - highest)
    scale_second = jnp.exp(second_part[0] - highest)
    seq_count, prop_count, head_count = highest.shape
    outer_first = (
        first_part[2].reshape(seq_count, prop_count, head_count, -1) * scale_first[..., None]
    )
    outer_second = (
        second_part[2].reshape(seq_count, prop_count, head_count, -1) * scale_second[..., None]
    )
    joined = (outer_first + outer_second).reshape(seq_count, prop_count, -1)
    return (highest, first_part[1] * scale_first + second_part[1] * scale_second, joined)


def local(
    tokens,
    norm_gain,
    w_query,
    w_key,
    w_value,
    w_forget,
    forget_bias,
    head_gain,
    w_out,
    cache_keys,
    cache_values,
    cache_gates,
    lengths,
    accepted,
    parents,
):
    seq_count, prop_count, model_width = tokens.shape
    span_rows = cache_keys.shape[1]
    head_count = cache_gates.shape[1]
    head_size = cache_keys.shape[2] // head_count
    scale = head_size ** (-0.5)
    start_pos = lax.axis_index("kv") * span_rows
    positions = start_pos + jnp.arange(span_rows, dtype=jnp.int32)
    valid_len = lengths + accepted
    flat_rows = tokens.reshape(seq_count * prop_count, model_width).astype(jnp.float32)
    normed = (
        flat_rows
        * lax.rsqrt(jnp.mean(flat_rows * flat_rows, axis=1, keepdims=True) + EPSILON)
        * norm_gain.astype(jnp.float32)
    ).astype(jnp.bfloat16)
    picked = (positions[None, :] == (valid_len - 1)[:, None]).astype(jnp.float32)
    last_part = jnp.sum(cache_gates * picked[:, None, :], axis=2)
    row_count = w_query.shape[0]
    own_columns = lax.dynamic_slice_in_dim(normed, lax.axis_index("kv") * row_count, row_count, 1)
    query_part = jnp.dot(own_columns, w_query, preferred_element_type=jnp.float32)
    key_part = jnp.dot(own_columns, w_key, preferred_element_type=jnp.float32)
    value_part = jnp.dot(own_columns, w_value, preferred_element_type=jnp.float32)
    gate_part = jnp.dot(own_columns, w_forget, preferred_element_type=jnp.float32)
    query, fresh_keys, fresh_values, gate_pre, last_gate = lax.psum(
        (query_part, key_part, value_part, gate_part, last_part), "kv"
    )
    query = query.astype(jnp.bfloat16).reshape(seq_count, prop_count, head_count, head_size)
    fresh_keys = fresh_keys.astype(jnp.bfloat16).reshape(
        seq_count, prop_count, head_count, head_size
    )
    fresh_values = fresh_values.astype(jnp.bfloat16).reshape(
        seq_count, prop_count, head_count, head_size
    )
    log_gate = jax.nn.log_sigmoid(gate_pre + forget_bias).reshape(seq_count, prop_count, head_count)
    link = ancestry(parents)
    climb = jnp.einsum("bia,bah->bih", link, log_gate, precision=lax.Precision.HIGHEST)
    stored_keys = cache_keys.reshape(seq_count, span_rows, head_count, head_size)
    stored_values = cache_values.reshape(seq_count, span_rows, head_count, head_size)
    scores = (
        jnp.einsum("bphd,bchd->bphc", query, stored_keys, preferred_element_type=jnp.float32)
        * scale
    )
    scores = scores + (last_gate[:, None, :] + climb)[..., None] - cache_gates[:, None]
    seen = (positions[None, :] < valid_len[:, None])[:, None, None, :]
    highest = jnp.max(jnp.where(seen, scores, NEG_LARGE), axis=3)
    weights = jnp.where(seen, jnp.exp(scores - highest[..., None]), 0.0)
    normalizer = jnp.sum(weights, axis=3)
    weighted = jnp.einsum(
        "bphc,bchd->bphd",
        weights.astype(jnp.bfloat16),
        stored_values,
        preferred_element_type=jnp.float32,
    )
    highest, normalizer, weighted = joined_2(
        (highest, normalizer, weighted.reshape(seq_count, prop_count, head_count * head_size)),
        "kv",
        merge_pair,
    )
    near_scores = (
        jnp.einsum("bphd,bahd->bpha", query, fresh_keys, preferred_element_type=jnp.float32) * scale
    )
    near_scores = near_scores + climb[..., None] - jnp.transpose(climb, (0, 2, 1))[:, None]
    linked = (link > 0.5)[:, :, None, :]
    near_high = jnp.max(jnp.where(linked, near_scores, NEG_LARGE), axis=3)
    overall = jnp.maximum(highest, near_high)
    carried = jnp.exp(highest - overall)
    near_weights = jnp.where(linked, jnp.exp(near_scores - overall[..., None]), 0.0)
    normalizer = normalizer * carried + jnp.sum(near_weights, axis=3)
    attended = weighted.reshape(seq_count, prop_count, head_count, head_size) * carried[..., None]
    attended = attended + jnp.einsum(
        "bpha,bahd->bphd",
        near_weights.astype(jnp.bfloat16),
        fresh_values,
        preferred_element_type=jnp.float32,
    )
    attended = attended / normalizer[..., None]
    gain_rows = head_gain.astype(jnp.float32).reshape(head_count, head_size)
    heads_out = (
        (
            attended
            * lax.rsqrt(jnp.mean(attended * attended, axis=3, keepdims=True) + EPSILON)
            * gain_rows
        )
        .astype(jnp.bfloat16)
        .reshape(seq_count * prop_count, head_count * head_size)
    )
    partial_sum = jnp.dot(heads_out, w_out, preferred_element_type=jnp.float32)
    summed = lax.psum_scatter(partial_sum, "tp", scatter_dimension=1, tiled=True)
    mixed = summed.reshape(seq_count, prop_count, -1)
    offsets = positions[None, :, None] - valid_len[:, None, None]
    placed = offsets == jnp.arange(prop_count, dtype=jnp.int32)[None, None, :]
    landed = jnp.any(placed, axis=2)
    placed_low = placed.astype(jnp.bfloat16)
    written_keys = jnp.einsum(
        "bcj,bjx->bcx",
        placed_low,
        fresh_keys.reshape(seq_count, prop_count, -1),
        preferred_element_type=jnp.float32,
    ).astype(jnp.bfloat16)
    written_values = jnp.einsum(
        "bcj,bjx->bcx",
        placed_low,
        fresh_values.reshape(seq_count, prop_count, -1),
        preferred_element_type=jnp.float32,
    ).astype(jnp.bfloat16)
    keys_out = jnp.where(landed[..., None], written_keys, cache_keys)
    values_out = jnp.where(landed[..., None], written_values, cache_values)
    new_gates = last_gate[:, :, None] + jnp.transpose(climb, (0, 2, 1))
    written_gates = jnp.einsum(
        "bcj,bhj->bhc", placed.astype(jnp.float32), new_gates, precision=lax.Precision.HIGHEST
    )
    gates_out = jnp.where(landed[:, None, :], written_gates, cache_gates)
    return (mixed, keys_out, values_out, gates_out)


HIGHEST = lax.Precision.HIGHEST
MESH = pl.DeviceIdType.MESH
LANES = 128
WINDOW = 16
VMEM_ALL = 67043328


def dot_rows(left, right, precision=None):
    return lax.dot_general(
        left,
        right,
        (((1,), (1,)), ((), ())),
        precision=precision,
        preferred_element_type=jnp.float32,
    )


def dot_plain(left, right, precision=None):
    return jnp.dot(left, right, precision=precision, preferred_element_type=jnp.float32)


def exchange_kernel(
    kv_count,
    head_count,
    lengths_ref,
    accepted_ref,
    tokens_hbm,
    gain_hbm,
    wq_hbm,
    wk_hbm,
    wv_hbm,
    wf_hbm,
    bias_hbm,
    head_gain_hbm,
    wo_hbm,
    keys_hbm,
    values_hbm,
    gates_hbm,
    parents_hbm,
    mixed_out,
    fresh_out,
    fresh_gates_out,
    tokens_ref,
    gain_ref,
    wq_ref,
    wk_ref,
    wv_ref,
    wf_ref,
    bias_ref,
    head_gain_ref,
    wo_ref,
    keys_ref,
    values_ref,
    gates_ref,
    parents_ref,
    q_send,
    q_recv,
    q_all,
    kv_send,
    kv_recv,
    kv_all,
    g_send,
    g_recv,
    g_all,
    w_send,
    w_recv,
    st_send,
    st_recv,
    h_all,
    o_send,
    o_recv,
    gain_wide,
    load_sem,
    send_sem,
    recv_sem,
    pair_sem,
):
    dp, me, tp = lax.axis_index("dp"), lax.axis_index("kv"), lax.axis_index("tp")
    seq_count, prop, _ = tokens_ref.shape
    depth, width = wq_ref.shape
    span = keys_ref.shape[1]
    head_size = width // head_count
    scale = head_size ** (-0.5)
    rows_all = head_count * prop
    half = wo_ref.shape[1] // 2
    offsets = range(1, kv_count)

    sources = (
        (tokens_hbm, tokens_ref),
        (gain_hbm, gain_ref),
        (wq_hbm, wq_ref),
        (wk_hbm, wk_ref),
        (wv_hbm, wv_ref),
        (wf_hbm, wf_ref),
        (gates_hbm, gates_ref),
        (keys_hbm, keys_ref),
        (values_hbm, values_ref),
        (parents_hbm, parents_ref),
        (bias_hbm, bias_ref),
        (head_gain_hbm, head_gain_ref),
        (wo_hbm, wo_ref),
    )
    loads = {}
    for at, (source, target) in enumerate(sources):
        copy = pltpu.make_async_copy(source, target, load_sem.at[at])
        copy.start()
        loads[id(target)] = copy

    def loaded(*refs):
        for ref in refs:
            loads[id(ref)].wait()

    barrier = pltpu.get_barrier_semaphore()
    for offset in offsets:
        pl.semaphore_signal(
            barrier,
            inc=1,
            device_id=(dp, lax.rem(me + offset, kv_count), tp),
            device_id_type=MESH,
        )
    pl.semaphore_signal(barrier, inc=1, device_id=(dp, me, 1 - tp), device_id_type=MESH)

    started = []

    def send(kind, offset, source, target):
        copy = pltpu.make_async_remote_copy(
            src_ref=source,
            dst_ref=target,
            send_sem=send_sem.at[kind, offset],
            recv_sem=recv_sem.at[kind, offset],
            device_id=(dp, lax.rem(me + offset, kv_count), tp),
            device_id_type=MESH,
        )
        copy.start()
        started.append(copy)
        return copy

    loaded(tokens_ref, gain_ref)
    flat = jnp.concatenate([tokens_ref[s].astype(jnp.float32) for s in range(seq_count)], 0)
    inverse = lax.rsqrt(jnp.mean(flat * flat, axis=1, keepdims=True) + EPSILON)
    start = pl.multiple_of(me * depth, depth)
    own = jnp.concatenate(
        [tokens_ref[s, :, pl.ds(start, depth)].astype(jnp.float32) for s in range(seq_count)], 0
    )
    gain_wide[...] = gain_ref[...].astype(jnp.float32)
    gain_rows = depth // LANES
    own_gain = jnp.concatenate(
        [gain_wide[pl.ds(me * gain_rows + at, 1), :] for at in range(gain_rows)], 1
    )
    normed = (own * inverse * own_gain).astype(jnp.bfloat16)
    loaded(wq_ref)
    q_part = dot_plain(normed, wq_ref[...])
    for s in range(seq_count):
        q_send[s] = q_part[s * prop : (s + 1) * prop]
    pl.semaphore_wait(barrier, kv_count)
    q_copies = [
        send(0, offset, q_send.at[lax.rem(me + offset, kv_count)], q_recv.at[offset])
        for offset in offsets
    ]

    loaded(wk_ref, wv_ref, wf_ref, gates_ref)
    k_part = dot_plain(normed, wk_ref[...])
    v_part = dot_plain(normed, wv_ref[...])
    f_part = dot_rows(wf_ref[...], normed)
    lane_pos = lax.broadcasted_iota(jnp.int32, (head_count, span), 1) + me * span
    for s in range(seq_count):
        rows = slice(s * prop, (s + 1) * prop)
        kv_send[s, 0] = k_part[rows].astype(jnp.bfloat16)
        kv_send[s, 1] = v_part[rows].astype(jnp.bfloat16)
        valid = lengths_ref[s] + accepted_ref[s]
        picked = jnp.where(lane_pos == valid - 1, gates_ref[s], 0.0)
        last = jnp.sum(picked, axis=1, keepdims=True)
        g_send[s] = jnp.broadcast_to(last, (head_count, LANES))
        g_send[s, :, :prop] = f_part[:, rows]

    loaded(parents_ref)
    parent_row = parents_ref[pl.ds(me, 1), :]
    up = lax.broadcasted_iota(jnp.int32, (prop, prop), 0)
    down = lax.broadcasted_iota(jnp.int32, (prop, prop), 1)
    eye = (up == down).astype(jnp.bfloat16)
    linked = jnp.where((up == parent_row) | (up == down), 1.0, 0.0)
    for repeat in range(prop.bit_length()):
        low = linked.astype(jnp.bfloat16)
        linked = jnp.minimum(dot_plain(low, low), 1.0)
    link = dot_rows(eye, linked.astype(jnp.bfloat16))

    total = q_send[me]
    for copy, offset in zip(q_copies, offsets):
        copy.wait_recv()
        total = total + q_recv[offset]
    q_all[me] = total.astype(jnp.bfloat16)
    qa_copies = {offset: send(1, offset, q_all.at[me], q_all.at[me]) for offset in offsets}
    kv_copies = []
    for offset in offsets:
        there = lax.rem(me + offset, kv_count)
        kv_copies.append(send(2, offset, kv_send.at[there], kv_recv.at[offset]))
        kv_copies.append(send(3, offset, g_send.at[there], g_recv.at[offset]))

    shape = (head_count, prop, width)
    head_mask = (
        lax.broadcasted_iota(jnp.int32, shape, 2) // head_size
        == lax.broadcasted_iota(jnp.int32, shape, 0)
    )
    small = (head_count, prop, LANES)
    small_lane = lax.broadcasted_iota(jnp.int32, small, 2)
    small_prop = lax.broadcasted_iota(jnp.int32, small, 1)

    def spread(query):
        wide = jnp.broadcast_to(query.astype(jnp.float32)[None], shape)
        return jnp.where(head_mask, wide, 0.0).reshape(rows_all, width).astype(jnp.bfloat16)

    def fold(wide):
        return jnp.sum(jnp.where(head_mask, wide.reshape(shape), 0.0), axis=0)

    def expand(column):
        return fold(jnp.broadcast_to(column, (rows_all, width)))

    def column_of(compact, first_lane):
        wide = jnp.broadcast_to(compact[:, None, :], small)
        taken = jnp.where(small_lane == small_prop + first_lane, wide, 0.0)
        return jnp.sum(taken.reshape(rows_all, LANES), axis=1, keepdims=True)

    score_pos = lax.broadcasted_iota(jnp.int32, (rows_all, span), 1) + me * span

    def attend(s):
        valid = lengths_ref[s] + accepted_ref[s]
        scores = dot_rows(spread(q_all[s]), keys_ref[s]) * scale
        gates = jnp.broadcast_to(gates_ref[s][:, None, :], (head_count, prop, span))
        scores = scores - gates.reshape(rows_all, span)
        seen = score_pos < valid
        highest = jnp.max(jnp.where(seen, scores, NEG_LARGE), axis=1, keepdims=True)
        weights = jnp.where(seen, jnp.exp(scores - highest), 0.0)
        normalizer = jnp.sum(weights, axis=1, keepdims=True)
        w_send[s] = fold(dot_plain(weights.astype(jnp.bfloat16), values_ref[s])).astype(
            jnp.bfloat16
        )
        both = jnp.where(
            small_lane == small_prop,
            highest.reshape(head_count, prop, 1),
            jnp.where(
                small_lane == small_prop + prop,
                normalizer.reshape(head_count, prop, 1),
                0.0,
            ),
        )
        st_send[s] = jnp.sum(both, axis=1)

    loaded(keys_ref, values_ref)
    attend(me)
    w_copies = {}
    for offset in offsets:
        qa_copies[offset].wait_recv()
        back = kv_count - offset
        there = lax.rem(me + back, kv_count)
        attend(there)
        w_copies[back] = (
            send(4, back, w_send.at[there], w_recv.at[back]),
            send(5, back, st_send.at[there], st_recv.at[back]),
        )

    for copy in kv_copies:
        copy.wait_recv()
    fresh_k = kv_send[me, 0].astype(jnp.float32)
    fresh_v = kv_send[me, 1].astype(jnp.float32)
    gate_sum = g_send[me]
    for offset in offsets:
        fresh_k = fresh_k + kv_recv[offset, 0].astype(jnp.float32)
        fresh_v = fresh_v + kv_recv[offset, 1].astype(jnp.float32)
        gate_sum = gate_sum + g_recv[offset]
    fresh_k = fresh_k.astype(jnp.bfloat16)
    fresh_v = fresh_v.astype(jnp.bfloat16)
    kv_all[me, 0] = fresh_k
    kv_all[me, 1] = fresh_v
    loaded(bias_ref)
    square = (head_count, head_count)
    on_diagonal = lax.broadcasted_iota(jnp.int32, square, 0) == lax.broadcasted_iota(
        jnp.int32, square, 1
    )
    bias = jnp.sum(
        jnp.where(on_diagonal, jnp.broadcast_to(bias_ref[...], square), 0.0), axis=1, keepdims=True
    )
    gate_pre = gate_sum[:, :prop] + bias
    log_gate = -(jnp.maximum(-gate_pre, 0.0) + jnp.log1p(jnp.exp(-jnp.abs(gate_pre))))
    climb_rows = dot_plain(log_gate, linked, HIGHEST)
    g_all[me] = jnp.zeros((head_count, LANES), jnp.float32)
    g_all[me, :, :prop] = gate_sum[:, prop : prop + 1] + climb_rows
    climb_wide = jnp.broadcast_to(climb_rows[:, None, :], (head_count, prop, prop))
    climb_col = jnp.sum(
        jnp.where((up == down)[None], climb_wide, 0.0).reshape(rows_all, prop),
        axis=1,
        keepdims=True,
    )
    near_shape = (head_count, prop, prop)
    near = dot_rows(spread(q_all[me]), fresh_k) * scale + climb_col
    near = near - climb_wide.reshape(rows_all, prop)
    near_link = jnp.broadcast_to(link[None], near_shape).reshape(rows_all, prop) > 0.5
    near_high = jnp.max(jnp.where(near_link, near, NEG_LARGE), axis=1, keepdims=True)
    near_weights = jnp.where(near_link, jnp.exp(near - near_high), 0.0)
    near_sum = jnp.sum(near_weights, axis=1, keepdims=True)
    near_wide = dot_plain(near_weights.astype(jnp.bfloat16), fresh_v)
    last_col = jnp.broadcast_to(
        gate_sum[:, prop : prop + 1][:, None, :], (head_count, prop, 1)
    ).reshape(rows_all, 1)
    shift = last_col + climb_col

    loaded(head_gain_ref)
    head_gain = head_gain_ref[...].astype(jnp.float32)
    for pair in w_copies.values():
        for copy in pair:
            copy.wait_recv()
    stats = [st_send[me]] + [st_recv[offset] for offset in offsets]
    parts = [w_send[me]] + [w_recv[offset] for offset in offsets]
    highs = [column_of(stat, 0) + shift for stat in stats]
    sums = [column_of(stat, prop) for stat in stats]
    overall = near_high
    for high in highs:
        overall = jnp.maximum(overall, high)
    near_factor = jnp.exp(near_high - overall)
    factors = [jnp.exp(high - overall) for high in highs]
    normalizer = near_sum * near_factor
    for factor, part in zip(factors, sums):
        normalizer = normalizer + factor * part
    attended = fold(near_wide * (near_factor / normalizer))
    for factor, part in zip(factors, parts):
        attended = attended + expand(factor / normalizer) * part.astype(jnp.float32)
    squares = jnp.where(head_mask, jnp.broadcast_to((attended * attended)[None], shape), 0.0)
    square_col = jnp.sum(squares.reshape(rows_all, width), axis=1, keepdims=True)
    rooted = lax.rsqrt(square_col * (1.0 / head_size) + EPSILON)
    head_out = attended * expand(rooted) * jnp.concatenate(
        [head_gain[at : at + 1] for at in range(width // LANES)], 1
    )
    h_all[me] = head_out.astype(jnp.bfloat16)
    h_copies = [send(6, offset, h_all.at[me], h_all.at[me]) for offset in offsets]
    fresh_copies = []
    for offset in offsets:
        fresh_copies.append(send(7, offset, kv_all.at[me], kv_all.at[me]))
        fresh_copies.append(send(8, offset, g_all.at[me], g_all.at[me]))

    loaded(wo_ref)
    for copy in h_copies:
        copy.wait_recv()
    heads = jnp.concatenate(
        [h_all[s].astype(jnp.float32) for s in range(seq_count)], 0
    ).astype(jnp.bfloat16)
    there = pl.multiple_of((1 - tp) * half, half)
    here = pl.multiple_of(tp * half, half)
    o_send[...] = dot_plain(heads, wo_ref[:, pl.ds(there, half)])
    pair = pltpu.make_async_remote_copy(
        src_ref=o_send,
        dst_ref=o_recv,
        send_sem=pair_sem.at[0],
        recv_sem=pair_sem.at[1],
        device_id=(dp, me, 1 - tp),
        device_id_type=MESH,
    )
    pair.start()
    own_sum = dot_plain(heads, wo_ref[:, pl.ds(here, half)])
    pair.wait()
    own_sum = own_sum + o_recv[...]
    for s in range(seq_count):
        mixed_out[s] = own_sum[s * prop : (s + 1) * prop]
    for copy in fresh_copies:
        copy.wait_recv()
    fresh_out[...] = kv_all[...]
    fresh_gates_out[...] = g_all[...]
    for copy in started:
        copy.wait_send()


def write_kernel(
    lengths_ref,
    accepted_ref,
    mixed_ref,
    fresh_ref,
    fresh_gates_ref,
    keys_hbm,
    values_hbm,
    gates_hbm,
    mixed_out,
    keys_out,
    values_out,
    gates_out,
    keys_ref,
    values_ref,
    gates_ref,
    read_sem,
    write_sem,
):
    seq_count, span, _ = keys_ref.shape
    prop = fresh_ref.shape[2]
    head_count = gates_ref.shape[1]
    rows = -(-(prop + WINDOW - 1) // WINDOW) * WINDOW
    reads = []
    for s in range(seq_count):
        triple = (
            pltpu.make_async_copy(keys_hbm.at[s], keys_ref.at[s], read_sem.at[0, s]),
            pltpu.make_async_copy(values_hbm.at[s], values_ref.at[s], read_sem.at[1, s]),
            pltpu.make_async_copy(gates_hbm.at[s], gates_ref.at[s], read_sem.at[2, s]),
        )
        for copy in triple:
            copy.start()
        reads.append(triple)
    writes = [pltpu.make_async_copy(mixed_ref, mixed_out, write_sem.at[3, 0])]
    writes[0].start()
    for s in range(seq_count):
        valid = lengths_ref[s] + accepted_ref[s]
        first = valid - lax.axis_index("kv") * span
        window = jnp.clip(first // WINDOW * WINDOW, 0, span - rows)
        window = pl.multiple_of(window, WINDOW)
        down = lax.broadcasted_iota(jnp.int32, (rows, prop), 0) + (window - first)
        placed = (down == lax.broadcasted_iota(jnp.int32, (rows, prop), 1)).astype(jnp.bfloat16)
        row = lax.broadcasted_iota(jnp.int32, (rows, keys_ref.shape[2]), 0) + (window - first)
        landed = (row >= 0) & (row < prop)
        over = lax.broadcasted_iota(jnp.int32, (prop, span), 1) - first
        spot = (over == lax.broadcasted_iota(jnp.int32, (prop, span), 0)).astype(jnp.float32)
        new_gates = dot_plain(fresh_gates_ref[s][:, :prop], spot, HIGHEST)
        lane = lax.broadcasted_iota(jnp.int32, (head_count, span), 1) - first
        for at, (target, out) in enumerate(((keys_ref, keys_out), (values_ref, values_out))):
            written = dot_plain(placed, fresh_ref[s, at])
            reads[s][at].wait()
            old = target[s, pl.ds(window, rows), :].astype(jnp.float32)
            target[s, pl.ds(window, rows), :] = jnp.where(landed, written, old).astype(
                jnp.bfloat16
            )
            writes.append(pltpu.make_async_copy(target.at[s], out.at[s], write_sem.at[at, s]))
            writes[-1].start()
        reads[s][2].wait()
        gates_ref[s] = jnp.where((lane >= 0) & (lane < prop), new_gates, gates_ref[s])
        writes.append(pltpu.make_async_copy(gates_ref.at[s], gates_out.at[s], write_sem.at[2, s]))
        writes[-1].start()
    for copy in writes:
        copy.wait()


def fused(
    kv_count,
    tokens,
    norm_gain,
    w_query,
    w_key,
    w_value,
    w_forget,
    forget_bias,
    head_gain,
    w_out,
    cache_keys,
    cache_values,
    cache_gates,
    lengths,
    accepted,
    parents,
):
    seq_count, prop, _ = tokens.shape
    span, width = cache_keys.shape[1:]
    head_count = cache_gates.shape[1]
    half = w_out.shape[1] // 2
    gain = norm_gain.reshape(-1, LANES)
    w_forget = w_forget.T
    bias = forget_bias.reshape(1, -1)
    head_gain = head_gain.reshape(-1, LANES)
    low, high = jnp.bfloat16, jnp.float32
    large = (
        tokens, gain, w_query, w_key, w_value, w_forget, bias, head_gain, w_out,
        cache_keys, cache_values, cache_gates, parents,
    )
    vmem = pltpu.VMEM
    scratch = [vmem(value.shape, value.dtype) for value in large]
    block = (seq_count, prop, width)
    pair = (seq_count, 2, prop, width)
    scratch += [
        vmem(block, high),
        vmem(block, high),
        vmem(block, low),
        vmem(pair, low),
        vmem(pair, low),
        vmem(pair, low),
        vmem((seq_count, head_count, LANES), high),
        vmem((seq_count, head_count, LANES), high),
        vmem((seq_count, head_count, LANES), high),
        vmem(block, low),
        vmem(block, low),
        vmem((seq_count, head_count, LANES), high),
        vmem((seq_count, head_count, LANES), high),
        vmem(block, low),
        vmem((seq_count * prop, half), high),
        vmem((seq_count * prop, half), high),
        vmem(gain.shape, high),
        pltpu.SemaphoreType.DMA((len(large),)),
        pltpu.SemaphoreType.DMA((9, kv_count)),
        pltpu.SemaphoreType.DMA((9, kv_count)),
        pltpu.SemaphoreType.DMA((2,)),
    ]
    kept = seq_count * (prop * half * 4 + 2 * prop * width * 2 + head_count * LANES * 4)
    smem = pl.BlockSpec(memory_space=pltpu.SMEM)
    mixed, fresh, fresh_gates = pl.pallas_call(
        functools.partial(exchange_kernel, kv_count, head_count),
        out_shape=(
            pltpu.VMEM((seq_count, prop, half), high),
            pltpu.VMEM(pair, low),
            pltpu.VMEM((seq_count, head_count, LANES), high),
        ),
        in_specs=[smem, smem] + [pl.BlockSpec(memory_space=pltpu.HBM)] * len(large),
        out_specs=(pl.BlockSpec(memory_space=pltpu.VMEM),) * 3,
        scratch_shapes=scratch,
        compiler_params=pltpu.CompilerParams(
            collective_id=0, has_side_effects=True, vmem_limit_bytes=VMEM_ALL - kept
        ),
        name="exchange",
    )(lengths, accepted, *large)

    held = pl.BlockSpec(memory_space=pltpu.VMEM)
    far = pl.BlockSpec(memory_space=pltpu.HBM)
    return pl.pallas_call(
        write_kernel,
        out_shape=(
            jax.ShapeDtypeStruct(mixed.shape, high),
            jax.ShapeDtypeStruct(cache_keys.shape, low),
            jax.ShapeDtypeStruct(cache_values.shape, low),
            jax.ShapeDtypeStruct(cache_gates.shape, high),
        ),
        in_specs=[smem, smem, held, held, held, far, far, far],
        out_specs=(far,) * 4,
        scratch_shapes=[
            vmem(cache_keys.shape, low),
            vmem(cache_values.shape, low),
            vmem(cache_gates.shape, high),
            pltpu.SemaphoreType.DMA((3, seq_count)),
            pltpu.SemaphoreType.DMA((4, seq_count)),
        ],
        compiler_params=pltpu.CompilerParams(vmem_limit_bytes=VMEM_ALL - kept),
        name="write",
    )(lengths, accepted, mixed, fresh, fresh_gates, cache_keys, cache_values, cache_gates)


def span_fits(*rest):
    depth, width = rest[1].shape
    span = rest[8].shape[1]
    return span % WINDOW == span % LANES == depth % LANES == width % LANES == 0


def device_step(kv_count, tp_count, tokens, *rest):
    seq_count, prop, _ = tokens.shape
    head_count = rest[10].shape[1]
    fits = seq_count == kv_count and tp_count == 2 and prop % 8 == 0 and 2 * prop <= LANES
    if fits and kv_count > 1 and head_count % 8 == 0 and span_fits(*rest):
        return fused(kv_count, tokens, *rest)
    return local(tokens, *rest)


def solution(mesh):
    placed = (
        P("dp", None, None),
        P(),
        P("kv", "tp"),
        P("kv", "tp"),
        P("kv", "tp"),
        P("kv", "tp"),
        P("tp"),
        P("tp"),
        P("tp", "kv"),
        P("dp", "kv", "tp"),
        P("dp", "kv", "tp"),
        P("dp", "tp", "kv"),
        P("dp"),
        P("dp"),
        P("dp", None),
    )
    return jax.shard_map(
        functools.partial(device_step, mesh.shape["kv"], mesh.shape["tp"]),
        mesh=mesh,
        in_specs=placed,
        out_specs=(
            P("dp", None, ("kv", "tp")),
            P("dp", "kv", "tp"),
            P("dp", "kv", "tp"),
            P("dp", "tp", "kv"),
        ),
        check_vma=False,
    )
```

```python
import functools

import jax
import jax.numpy as jnp
from jax import lax
from jax.experimental import pallas as pl
from jax.experimental.pallas import tpu as pltpu
from jax.sharding import PartitionSpec as P

NEG_LARGE = -1e30
EPSILON = 1e-06


def joined_2(value, axis, join):
    pieces = jax.tree.map(lambda part: lax.all_gather(part, axis), value)
    head = jax.tree.map(lambda part: part[0], pieces)
    tail = jax.tree.map(lambda part: part[1:], pieces)
    total, _ = lax.scan(lambda total, piece: (join(total, piece), None), head, tail)
    return total


def ancestry(parents):
    prop_count = parents.shape[1]
    indices = jnp.arange(prop_count, dtype=jnp.int32)
    linked = (parents[:, :, None] == indices[None, None, :]).astype(jnp.float32)
    linked = linked + (indices[:, None] == indices[None, :]).astype(jnp.float32)[None]
    for repeat in range(prop_count.bit_length()):
        linked = jnp.minimum(
            jnp.einsum("bij,bjk->bik", linked, linked, precision=lax.Precision.HIGHEST), 1.0
        )
    return linked


def merge_pair(first_part, second_part):
    highest = jnp.maximum(first_part[0], second_part[0])
    scale_first = jnp.exp(first_part[0] - highest)
    scale_second = jnp.exp(second_part[0] - highest)
    seq_count, prop_count, head_count = highest.shape
    outer_first = (
        first_part[2].reshape(seq_count, prop_count, head_count, -1) * scale_first[..., None]
    )
    outer_second = (
        second_part[2].reshape(seq_count, prop_count, head_count, -1) * scale_second[..., None]
    )
    joined = (outer_first + outer_second).reshape(seq_count, prop_count, -1)
    return (highest, first_part[1] * scale_first + second_part[1] * scale_second, joined)


def local(
    tokens,
    norm_gain,
    w_query,
    w_key,
    w_value,
    w_forget,
    forget_bias,
    head_gain,
    w_out,
    cache_keys,
    cache_values,
    cache_gates,
    lengths,
    accepted,
    parents,
):
    seq_count, prop_count, model_width = tokens.shape
    span_rows = cache_keys.shape[1]
    head_count = cache_gates.shape[1]
    head_size = cache_keys.shape[2] // head_count
    scale = head_size ** (-0.5)
    start_pos = lax.axis_index("kv") * span_rows
    positions = start_pos + jnp.arange(span_rows, dtype=jnp.int32)
    valid_len = lengths + accepted
    flat_rows = tokens.reshape(seq_count * prop_count, model_width).astype(jnp.float32)
    normed = (
        flat_rows
        * lax.rsqrt(jnp.mean(flat_rows * flat_rows, axis=1, keepdims=True) + EPSILON)
        * norm_gain.astype(jnp.float32)
    ).astype(jnp.bfloat16)
    picked = (positions[None, :] == (valid_len - 1)[:, None]).astype(jnp.float32)
    last_part = jnp.sum(cache_gates * picked[:, None, :], axis=2)
    row_count = w_query.shape[0]
    own_columns = lax.dynamic_slice_in_dim(normed, lax.axis_index("kv") * row_count, row_count, 1)
    query_part = jnp.dot(own_columns, w_query, preferred_element_type=jnp.float32)
    key_part = jnp.dot(own_columns, w_key, preferred_element_type=jnp.float32)
    value_part = jnp.dot(own_columns, w_value, preferred_element_type=jnp.float32)
    gate_part = jnp.dot(own_columns, w_forget, preferred_element_type=jnp.float32)
    query, fresh_keys, fresh_values, gate_pre, last_gate = lax.psum(
        (query_part, key_part, value_part, gate_part, last_part), "kv"
    )
    query = query.astype(jnp.bfloat16).reshape(seq_count, prop_count, head_count, head_size)
    fresh_keys = fresh_keys.astype(jnp.bfloat16).reshape(
        seq_count, prop_count, head_count, head_size
    )
    fresh_values = fresh_values.astype(jnp.bfloat16).reshape(
        seq_count, prop_count, head_count, head_size
    )
    log_gate = jax.nn.log_sigmoid(gate_pre + forget_bias).reshape(seq_count, prop_count, head_count)
    link = ancestry(parents)
    climb = jnp.einsum("bia,bah->bih", link, log_gate, precision=lax.Precision.HIGHEST)
    stored_keys = cache_keys.reshape(seq_count, span_rows, head_count, head_size)
    stored_values = cache_values.reshape(seq_count, span_rows, head_count, head_size)
    scores = (
        jnp.einsum("bphd,bchd->bphc", query, stored_keys, preferred_element_type=jnp.float32)
        * scale
    )
    scores = scores + (last_gate[:, None, :] + climb)[..., None] - cache_gates[:, None]
    seen = (positions[None, :] < valid_len[:, None])[:, None, None, :]
    highest = jnp.max(jnp.where(seen, scores, NEG_LARGE), axis=3)
    weights = jnp.where(seen, jnp.exp(scores - highest[..., None]), 0.0)
    normalizer = jnp.sum(weights, axis=3)
    weighted = jnp.einsum(
        "bphc,bchd->bphd",
        weights.astype(jnp.bfloat16),
        stored_values,
        preferred_element_type=jnp.float32,
    )
    highest, normalizer, weighted = joined_2(
        (highest, normalizer, weighted.reshape(seq_count, prop_count, head_count * head_size)),
        "kv",
        merge_pair,
    )
    near_scores = (
        jnp.einsum("bphd,bahd->bpha", query, fresh_keys, preferred_element_type=jnp.float32) * scale
    )
    near_scores = near_scores + climb[..., None] - jnp.transpose(climb, (0, 2, 1))[:, None]
    linked = (link > 0.5)[:, :, None, :]
    near_high = jnp.max(jnp.where(linked, near_scores, NEG_LARGE), axis=3)
    overall = jnp.maximum(highest, near_high)
    carried = jnp.exp(highest - overall)
    near_weights = jnp.where(linked, jnp.exp(near_scores - overall[..., None]), 0.0)
    normalizer = normalizer * carried + jnp.sum(near_weights, axis=3)
    attended = weighted.reshape(seq_count, prop_count, head_count, head_size) * carried[..., None]
    attended = attended + jnp.einsum(
        "bpha,bahd->bphd",
        near_weights.astype(jnp.bfloat16),
        fresh_values,
        preferred_element_type=jnp.float32,
    )
    attended = attended / normalizer[..., None]
    gain_rows = head_gain.astype(jnp.float32).reshape(head_count, head_size)
    heads_out = (
        (
            attended
            * lax.rsqrt(jnp.mean(attended * attended, axis=3, keepdims=True) + EPSILON)
            * gain_rows
        )
        .astype(jnp.bfloat16)
        .reshape(seq_count * prop_count, head_count * head_size)
    )
    partial_sum = jnp.dot(heads_out, w_out, preferred_element_type=jnp.float32)
    summed = lax.psum_scatter(partial_sum, "tp", scatter_dimension=1, tiled=True)
    mixed = summed.reshape(seq_count, prop_count, -1)
    offsets = positions[None, :, None] - valid_len[:, None, None]
    placed = offsets == jnp.arange(prop_count, dtype=jnp.int32)[None, None, :]
    landed = jnp.any(placed, axis=2)
    placed_low = placed.astype(jnp.bfloat16)
    written_keys = jnp.einsum(
        "bcj,bjx->bcx",
        placed_low,
        fresh_keys.reshape(seq_count, prop_count, -1),
        preferred_element_type=jnp.float32,
    ).astype(jnp.bfloat16)
    written_values = jnp.einsum(
        "bcj,bjx->bcx",
        placed_low,
        fresh_values.reshape(seq_count, prop_count, -1),
        preferred_element_type=jnp.float32,
    ).astype(jnp.bfloat16)
    keys_out = jnp.where(landed[..., None], written_keys, cache_keys)
    values_out = jnp.where(landed[..., None], written_values, cache_values)
    new_gates = last_gate[:, :, None] + jnp.transpose(climb, (0, 2, 1))
    written_gates = jnp.einsum(
        "bcj,bhj->bhc", placed.astype(jnp.float32), new_gates, precision=lax.Precision.HIGHEST
    )
    gates_out = jnp.where(landed[:, None, :], written_gates, cache_gates)
    return (mixed, keys_out, values_out, gates_out)


HIGHEST = lax.Precision.HIGHEST
MESH = pl.DeviceIdType.MESH
LANES = 128
WINDOW = 16
VMEM_ALL = 67043328


def dot_rows(left, right, precision=None):
    return lax.dot_general(
        left,
        right,
        (((1,), (1,)), ((), ())),
        precision=precision,
        preferred_element_type=jnp.float32,
    )


def dot_plain(left, right, precision=None):
    return jnp.dot(left, right, precision=precision, preferred_element_type=jnp.float32)


def exchange_kernel(
    kv_count,
    head_count,
    lengths_ref,
    accepted_ref,
    tokens_hbm,
    gain_hbm,
    wq_hbm,
    wk_hbm,
    wv_hbm,
    wf_hbm,
    bias_hbm,
    head_gain_hbm,
    wo_hbm,
    keys_hbm,
    values_hbm,
    gates_hbm,
    parents_hbm,
    mixed_out,
    fresh_out,
    fresh_gates_out,
    keys_ref,
    values_ref,
    gates_ref,
    tokens_ref,
    gain_ref,
    wq_ref,
    wk_ref,
    wv_ref,
    wf_ref,
    bias_ref,
    head_gain_ref,
    wo_ref,
    parents_ref,
    q_send,
    q_recv,
    q_all,
    kv_send,
    kv_recv,
    kv_all,
    g_send,
    g_recv,
    g_all,
    w_send,
    w_recv,
    st_send,
    st_recv,
    h_all,
    o_send,
    o_recv,
    gain_wide,
    load_sem,
    send_sem,
    recv_sem,
    pair_sem,
):
    dp, me, tp = lax.axis_index("dp"), lax.axis_index("kv"), lax.axis_index("tp")
    seq_count, prop, _ = tokens_ref.shape
    depth, width = wq_ref.shape
    span = keys_ref.shape[1]
    head_size = width // head_count
    scale = head_size ** (-0.5)
    rows_all = head_count * prop
    half = wo_ref.shape[1] // 2
    offsets = range(1, kv_count)

    sources = (
        (tokens_hbm, tokens_ref),
        (gain_hbm, gain_ref),
        (wq_hbm, wq_ref),
        (wk_hbm, wk_ref),
        (wv_hbm, wv_ref),
        (wf_hbm, wf_ref),
        (gates_hbm, gates_ref),
        (keys_hbm, keys_ref),
        (values_hbm, values_ref),
        (parents_hbm, parents_ref),
        (bias_hbm, bias_ref),
        (head_gain_hbm, head_gain_ref),
        (wo_hbm, wo_ref),
    )
    loads = {}
    for at, (source, target) in enumerate(sources):
        copy = pltpu.make_async_copy(source, target, load_sem.at[at])
        copy.start()
        loads[id(target)] = copy

    def loaded(*refs):
        for ref in refs:
            loads[id(ref)].wait()

    barrier = pltpu.get_barrier_semaphore()
    for offset in offsets:
        pl.semaphore_signal(
            barrier,
            inc=1,
            device_id=(dp, lax.rem(me + offset, kv_count), tp),
            device_id_type=MESH,
        )
    pl.semaphore_signal(barrier, inc=1, device_id=(dp, me, 1 - tp), device_id_type=MESH)

    started = []

    def send(kind, offset, source, target):
        copy = pltpu.make_async_remote_copy(
            src_ref=source,
            dst_ref=target,
            send_sem=send_sem.at[kind, offset],
            recv_sem=recv_sem.at[kind, offset],
            device_id=(dp, lax.rem(me + offset, kv_count), tp),
            device_id_type=MESH,
        )
        copy.start()
        started.append(copy)
        return copy

    loaded(tokens_ref, gain_ref)
    flat = jnp.concatenate([tokens_ref[s].astype(jnp.float32) for s in range(seq_count)], 0)
    inverse = lax.rsqrt(jnp.mean(flat * flat, axis=1, keepdims=True) + EPSILON)
    start = pl.multiple_of(me * depth, depth)
    own = jnp.concatenate(
        [tokens_ref[s, :, pl.ds(start, depth)].astype(jnp.float32) for s in range(seq_count)], 0
    )
    gain_wide[...] = gain_ref[...].astype(jnp.float32)
    gain_rows = depth // LANES
    own_gain = jnp.concatenate(
        [gain_wide[pl.ds(me * gain_rows + at, 1), :] for at in range(gain_rows)], 1
    )
    normed = (own * inverse * own_gain).astype(jnp.bfloat16)
    loaded(wq_ref)
    q_part = dot_plain(normed, wq_ref[...])
    for s in range(seq_count):
        q_send[s] = q_part[s * prop : (s + 1) * prop]
    pl.semaphore_wait(barrier, kv_count)
    q_copies = [
        send(0, offset, q_send.at[lax.rem(me + offset, kv_count)], q_recv.at[offset])
        for offset in offsets
    ]

    loaded(wk_ref, wv_ref, wf_ref, gates_ref)
    k_part = dot_plain(normed, wk_ref[...])
    v_part = dot_plain(normed, wv_ref[...])
    f_part = dot_rows(wf_ref[...], normed)
    lane_pos = lax.broadcasted_iota(jnp.int32, (head_count, span), 1) + me * span
    for s in range(seq_count):
        rows = slice(s * prop, (s + 1) * prop)
        kv_send[s, 0] = k_part[rows].astype(jnp.bfloat16)
        kv_send[s, 1] = v_part[rows].astype(jnp.bfloat16)
        valid = lengths_ref[s] + accepted_ref[s]
        picked = jnp.where(lane_pos == valid - 1, gates_ref[s], 0.0)
        last = jnp.sum(picked, axis=1, keepdims=True)
        g_send[s] = jnp.broadcast_to(last, (head_count, LANES))
        g_send[s, :, :prop] = f_part[:, rows]

    loaded(parents_ref)
    parent_row = parents_ref[pl.ds(me, 1), :]
    up = lax.broadcasted_iota(jnp.int32, (prop, prop), 0)
    down = lax.broadcasted_iota(jnp.int32, (prop, prop), 1)
    eye = (up == down).astype(jnp.bfloat16)
    linked = jnp.where((up == parent_row) | (up == down), 1.0, 0.0)
    for repeat in range(prop.bit_length()):
        low = linked.astype(jnp.bfloat16)
        linked = jnp.minimum(dot_plain(low, low), 1.0)
    link = dot_rows(eye, linked.astype(jnp.bfloat16))

    total = q_send[me]
    for copy, offset in zip(q_copies, offsets):
        copy.wait_recv()
        total = total + q_recv[offset]
    q_all[me] = total.astype(jnp.bfloat16)
    qa_copies = {offset: send(1, offset, q_all.at[me], q_all.at[me]) for offset in offsets}
    kv_copies = []
    for offset in offsets:
        there = lax.rem(me + offset, kv_count)
        kv_copies.append(send(2, offset, kv_send.at[there], kv_recv.at[offset]))
        kv_copies.append(send(3, offset, g_send.at[there], g_recv.at[offset]))

    shape = (head_count, prop, width)
    head_mask = (
        lax.broadcasted_iota(jnp.int32, shape, 2) // head_size
        == lax.broadcasted_iota(jnp.int32, shape, 0)
    )
    small = (head_count, prop, LANES)
    small_lane = lax.broadcasted_iota(jnp.int32, small, 2)
    small_prop = lax.broadcasted_iota(jnp.int32, small, 1)

    def spread(query):
        wide = jnp.broadcast_to(query.astype(jnp.float32)[None], shape)
        return jnp.where(head_mask, wide, 0.0).reshape(rows_all, width).astype(jnp.bfloat16)

    def fold(wide):
        return jnp.sum(jnp.where(head_mask, wide.reshape(shape), 0.0), axis=0)

    def expand(column):
        return fold(jnp.broadcast_to(column, (rows_all, width)))

    def column_of(compact, first_lane):
        wide = jnp.broadcast_to(compact[:, None, :], small)
        taken = jnp.where(small_lane == small_prop + first_lane, wide, 0.0)
        return jnp.sum(taken.reshape(rows_all, LANES), axis=1, keepdims=True)

    score_pos = lax.broadcasted_iota(jnp.int32, (rows_all, span), 1) + me * span

    def attend(s):
        valid = lengths_ref[s] + accepted_ref[s]
        scores = dot_rows(spread(q_all[s]), keys_ref[s]) * scale
        gates = jnp.broadcast_to(gates_ref[s][:, None, :], (head_count, prop, span))
        scores = scores - gates.reshape(rows_all, span)
        seen = score_pos < valid
        highest = jnp.max(jnp.where(seen, scores, NEG_LARGE), axis=1, keepdims=True)
        weights = jnp.where(seen, jnp.exp(scores - highest), 0.0)
        normalizer = jnp.sum(weights, axis=1, keepdims=True)
        w_send[s] = fold(dot_plain(weights.astype(jnp.bfloat16), values_ref[s])).astype(
            jnp.bfloat16
        )
        both = jnp.where(
            small_lane == small_prop,
            highest.reshape(head_count, prop, 1),
            jnp.where(
                small_lane == small_prop + prop,
                normalizer.reshape(head_count, prop, 1),
                0.0,
            ),
        )
        st_send[s] = jnp.sum(both, axis=1)

    loaded(keys_ref, values_ref)
    attend(me)
    w_copies = {}
    for offset in offsets:
        qa_copies[offset].wait_recv()
        back = kv_count - offset
        there = lax.rem(me + back, kv_count)
        attend(there)
        w_copies[back] = (
            send(4, back, w_send.at[there], w_recv.at[back]),
            send(5, back, st_send.at[there], st_recv.at[back]),
        )

    for copy in kv_copies:
        copy.wait_recv()
    fresh_k = kv_send[me, 0].astype(jnp.float32)
    fresh_v = kv_send[me, 1].astype(jnp.float32)
    gate_sum = g_send[me]
    for offset in offsets:
        fresh_k = fresh_k + kv_recv[offset, 0].astype(jnp.float32)
        fresh_v = fresh_v + kv_recv[offset, 1].astype(jnp.float32)
        gate_sum = gate_sum + g_recv[offset]
    fresh_k = fresh_k.astype(jnp.bfloat16)
    fresh_v = fresh_v.astype(jnp.bfloat16)
    kv_all[me, 0] = fresh_k
    kv_all[me, 1] = fresh_v
    loaded(bias_ref)
    square = (head_count, head_count)
    on_diagonal = lax.broadcasted_iota(jnp.int32, square, 0) == lax.broadcasted_iota(
        jnp.int32, square, 1
    )
    bias = jnp.sum(
        jnp.where(on_diagonal, jnp.broadcast_to(bias_ref[...], square), 0.0), axis=1, keepdims=True
    )
    gate_pre = gate_sum[:, :prop] + bias
    log_gate = -(jnp.maximum(-gate_pre, 0.0) + jnp.log1p(jnp.exp(-jnp.abs(gate_pre))))
    climb_rows = dot_plain(log_gate, linked, HIGHEST)
    g_all[me] = jnp.zeros((head_count, LANES), jnp.float32)
    g_all[me, :, :prop] = gate_sum[:, prop : prop + 1] + climb_rows
    climb_wide = jnp.broadcast_to(climb_rows[:, None, :], (head_count, prop, prop))
    climb_col = jnp.sum(
        jnp.where((up == down)[None], climb_wide, 0.0).reshape(rows_all, prop),
        axis=1,
        keepdims=True,
    )
    near_shape = (head_count, prop, prop)
    near = dot_rows(spread(q_all[me]), fresh_k) * scale + climb_col
    near = near - climb_wide.reshape(rows_all, prop)
    near_link = jnp.broadcast_to(link[None], near_shape).reshape(rows_all, prop) > 0.5
    near_high = jnp.max(jnp.where(near_link, near, NEG_LARGE), axis=1, keepdims=True)
    near_weights = jnp.where(near_link, jnp.exp(near - near_high), 0.0)
    near_sum = jnp.sum(near_weights, axis=1, keepdims=True)
    near_wide = dot_plain(near_weights.astype(jnp.bfloat16), fresh_v)
    last_col = jnp.broadcast_to(
        gate_sum[:, prop : prop + 1][:, None, :], (head_count, prop, 1)
    ).reshape(rows_all, 1)
    shift = last_col + climb_col

    loaded(head_gain_ref)
    head_gain = head_gain_ref[...].astype(jnp.float32)
    for pair in w_copies.values():
        for copy in pair:
            copy.wait_recv()
    stats = [st_send[me]] + [st_recv[offset] for offset in offsets]
    parts = [w_send[me]] + [w_recv[offset] for offset in offsets]
    highs = [column_of(stat, 0) + shift for stat in stats]
    sums = [column_of(stat, prop) for stat in stats]
    overall = near_high
    for high in highs:
        overall = jnp.maximum(overall, high)
    near_factor = jnp.exp(near_high - overall)
    factors = [jnp.exp(high - overall) for high in highs]
    normalizer = near_sum * near_factor
    for factor, part in zip(factors, sums):
        normalizer = normalizer + factor * part
    attended = fold(near_wide * (near_factor / normalizer))
    for factor, part in zip(factors, parts):
        attended = attended + expand(factor / normalizer) * part.astype(jnp.float32)
    squares = jnp.where(head_mask, jnp.broadcast_to((attended * attended)[None], shape), 0.0)
    square_col = jnp.sum(squares.reshape(rows_all, width), axis=1, keepdims=True)
    rooted = lax.rsqrt(square_col * (1.0 / head_size) + EPSILON)
    head_out = attended * expand(rooted) * jnp.concatenate(
        [head_gain[at : at + 1] for at in range(width // LANES)], 1
    )
    h_all[me] = head_out.astype(jnp.bfloat16)
    h_copies = [send(6, offset, h_all.at[me], h_all.at[me]) for offset in offsets]
    fresh_copies = []
    for offset in offsets:
        fresh_copies.append(send(7, offset, kv_all.at[me], kv_all.at[me]))
        fresh_copies.append(send(8, offset, g_all.at[me], g_all.at[me]))

    loaded(wo_ref)
    for copy in h_copies:
        copy.wait_recv()
    heads = jnp.concatenate(
        [h_all[s].astype(jnp.float32) for s in range(seq_count)], 0
    ).astype(jnp.bfloat16)
    there = pl.multiple_of((1 - tp) * half, half)
    here = pl.multiple_of(tp * half, half)
    o_send[...] = dot_plain(heads, wo_ref[:, pl.ds(there, half)])
    pair = pltpu.make_async_remote_copy(
        src_ref=o_send,
        dst_ref=o_recv,
        send_sem=pair_sem.at[0],
        recv_sem=pair_sem.at[1],
        device_id=(dp, me, 1 - tp),
        device_id_type=MESH,
    )
    pair.start()
    own_sum = dot_plain(heads, wo_ref[:, pl.ds(here, half)])
    pair.wait()
    own_sum = own_sum + o_recv[...]
    for s in range(seq_count):
        mixed_out[s] = own_sum[s * prop : (s + 1) * prop]
    for copy in fresh_copies:
        copy.wait_recv()
    fresh_out[...] = kv_all[...]
    fresh_gates_out[...] = g_all[...]
    for copy in started:
        copy.wait_send()


def write_kernel(
    lengths_ref,
    accepted_ref,
    mixed_ref,
    fresh_ref,
    fresh_gates_ref,
    keys_ref,
    values_ref,
    gates_ref,
    mixed_out,
    keys_out,
    values_out,
    gates_out,
    window_ref,
    new_gates_ref,
    bulk_sem,
    write_sem,
):
    seq_count, span, width = keys_ref.shape
    prop = fresh_ref.shape[2]
    head_count = gates_ref.shape[1]
    rows = window_ref.shape[2]
    caches = ((keys_ref, keys_out), (values_ref, values_out))
    bulk = [
        pltpu.make_async_copy(source, out, bulk_sem.at[at])
        for at, (source, out) in enumerate(caches + ((mixed_ref, mixed_out),))
    ]
    for copy in bulk:
        copy.start()
    starts = []
    for s in range(seq_count):
        valid = lengths_ref[s] + accepted_ref[s]
        first = valid - lax.axis_index("kv") * span
        window = jnp.clip(first // WINDOW * WINDOW, 0, span - rows)
        window = pl.multiple_of(window, WINDOW)
        starts.append(window)
        over = lax.broadcasted_iota(jnp.int32, (prop, span), 1) - first
        spot = (over == lax.broadcasted_iota(jnp.int32, (prop, span), 0)).astype(jnp.float32)
        new_gates = dot_plain(fresh_gates_ref[s][:, :prop], spot, HIGHEST)
        lane = lax.broadcasted_iota(jnp.int32, (head_count, span), 1) - first
        new_gates_ref[s] = jnp.where((lane >= 0) & (lane < prop), new_gates, gates_ref[s])
        down = lax.broadcasted_iota(jnp.int32, (rows, prop), 0) + (window - first)
        placed = (down == lax.broadcasted_iota(jnp.int32, (rows, prop), 1)).astype(jnp.bfloat16)
        row = lax.broadcasted_iota(jnp.int32, (rows, width), 0) + (window - first)
        landed = (row >= 0) & (row < prop)
        for at, (source, _) in enumerate(caches):
            written = dot_plain(placed, fresh_ref[s, at])
            old = source[s, pl.ds(window, rows), :].astype(jnp.float32)
            window_ref[at, s] = jnp.where(landed, written, old).astype(jnp.bfloat16)
    writes = [pltpu.make_async_copy(new_gates_ref, gates_out, write_sem.at[2, 0])]
    writes[0].start()
    for at, (_, out) in enumerate(caches):
        bulk[at].wait()
        for s in range(seq_count):
            writes.append(
                pltpu.make_async_copy(
                    window_ref.at[at, s],
                    out.at[s, pl.ds(starts[s], rows), :],
                    write_sem.at[at, s],
                )
            )
            writes[-1].start()
    bulk[2].wait()
    for copy in writes:
        copy.wait()


def fused(
    kv_count,
    tokens,
    norm_gain,
    w_query,
    w_key,
    w_value,
    w_forget,
    forget_bias,
    head_gain,
    w_out,
    cache_keys,
    cache_values,
    cache_gates,
    lengths,
    accepted,
    parents,
):
    seq_count, prop, _ = tokens.shape
    span, width = cache_keys.shape[1:]
    head_count = cache_gates.shape[1]
    half = w_out.shape[1] // 2
    gain = norm_gain.reshape(-1, LANES)
    w_forget = w_forget.T
    bias = forget_bias.reshape(1, -1)
    head_gain = head_gain.reshape(-1, LANES)
    low, high = jnp.bfloat16, jnp.float32
    large = (
        tokens, gain, w_query, w_key, w_value, w_forget, bias, head_gain, w_out,
        cache_keys, cache_values, cache_gates, parents,
    )
    vmem = pltpu.VMEM
    scratch = [vmem(value.shape, value.dtype) for value in large[:9] + large[12:]]
    block = (seq_count, prop, width)
    pair = (seq_count, 2, prop, width)
    scratch += [
        vmem(block, high),
        vmem(block, high),
        vmem(block, low),
        vmem(pair, low),
        vmem(pair, low),
        vmem(pair, low),
        vmem((seq_count, head_count, LANES), high),
        vmem((seq_count, head_count, LANES), high),
        vmem((seq_count, head_count, LANES), high),
        vmem(block, low),
        vmem(block, low),
        vmem((seq_count, head_count, LANES), high),
        vmem((seq_count, head_count, LANES), high),
        vmem(block, low),
        vmem((seq_count * prop, half), high),
        vmem((seq_count * prop, half), high),
        vmem(gain.shape, high),
        pltpu.SemaphoreType.DMA((len(large),)),
        pltpu.SemaphoreType.DMA((9, kv_count)),
        pltpu.SemaphoreType.DMA((9, kv_count)),
        pltpu.SemaphoreType.DMA((2,)),
    ]
    kept = seq_count * (
        prop * half * 4
        + 2 * (prop + span) * width * 2
        + head_count * (LANES + span) * 4
    )
    smem = pl.BlockSpec(memory_space=pltpu.SMEM)
    held_parts = pl.pallas_call(
        functools.partial(exchange_kernel, kv_count, head_count),
        out_shape=(
            pltpu.VMEM((seq_count, prop, half), high),
            pltpu.VMEM(pair, low),
            pltpu.VMEM((seq_count, head_count, LANES), high),
            pltpu.VMEM(cache_keys.shape, low),
            pltpu.VMEM(cache_values.shape, low),
            pltpu.VMEM(cache_gates.shape, high),
        ),
        in_specs=[smem, smem] + [pl.BlockSpec(memory_space=pltpu.HBM)] * len(large),
        out_specs=(pl.BlockSpec(memory_space=pltpu.VMEM),) * 6,
        scratch_shapes=scratch,
        compiler_params=pltpu.CompilerParams(
            collective_id=0, has_side_effects=True, vmem_limit_bytes=VMEM_ALL - kept
        ),
        name="exchange",
    )(lengths, accepted, *large)

    held = pl.BlockSpec(memory_space=pltpu.VMEM)
    rows = -(-(prop + WINDOW - 1) // WINDOW) * WINDOW
    far = pl.BlockSpec(memory_space=pltpu.HBM)
    return pl.pallas_call(
        write_kernel,
        out_shape=(
            jax.ShapeDtypeStruct((seq_count, prop, half), high),
            jax.ShapeDtypeStruct(cache_keys.shape, low),
            jax.ShapeDtypeStruct(cache_values.shape, low),
            jax.ShapeDtypeStruct(cache_gates.shape, high),
        ),
        in_specs=[smem, smem] + [held] * 6,
        out_specs=(far,) * 4,
        scratch_shapes=[
            vmem((2, seq_count, rows, width), low),
            vmem(cache_gates.shape, high),
            pltpu.SemaphoreType.DMA((3,)),
            pltpu.SemaphoreType.DMA((3, seq_count)),
        ],
        compiler_params=pltpu.CompilerParams(vmem_limit_bytes=8 * 1024 * 1024),
        name="write",
    )(lengths, accepted, *held_parts)


def span_fits(*rest):
    depth, width = rest[1].shape
    span = rest[8].shape[1]
    return span >= 4 * WINDOW and span % WINDOW == span % LANES == depth % LANES == width % LANES == 0


def device_step(kv_count, tp_count, tokens, *rest):
    seq_count, prop, _ = tokens.shape
    head_count = rest[10].shape[1]
    fits = seq_count == kv_count and tp_count == 2 and prop % 8 == 0 and 2 * prop <= LANES
    if fits and kv_count > 1 and head_count % 8 == 0 and span_fits(*rest):
        return fused(kv_count, tokens, *rest)
    return local(tokens, *rest)


def solution(mesh):
    placed = (
        P("dp", None, None),
        P(),
        P("kv", "tp"),
        P("kv", "tp"),
        P("kv", "tp"),
        P("kv", "tp"),
        P("tp"),
        P("tp"),
        P("tp", "kv"),
        P("dp", "kv", "tp"),
        P("dp", "kv", "tp"),
        P("dp", "tp", "kv"),
        P("dp"),
        P("dp"),
        P("dp", None),
    )
    return jax.shard_map(
        functools.partial(device_step, mesh.shape["kv"], mesh.shape["tp"]),
        mesh=mesh,
        in_specs=placed,
        out_specs=(
            P("dp", None, ("kv", "tp")),
            P("dp", "kv", "tp"),
            P("dp", "kv", "tp"),
            P("dp", "tp", "kv"),
        ),
        check_vma=False,
    )
```

```python
import functools

import jax
import jax.numpy as jnp
from jax import lax
from jax.experimental import pallas as pl
from jax.experimental.pallas import tpu as pltpu
from jax.sharding import PartitionSpec as P

NEG_LARGE = -1e30
EPSILON = 1e-06


def joined_2(value, axis, join):
    pieces = jax.tree.map(lambda part: lax.all_gather(part, axis), value)
    head = jax.tree.map(lambda part: part[0], pieces)
    tail = jax.tree.map(lambda part: part[1:], pieces)
    total, _ = lax.scan(lambda total, piece: (join(total, piece), None), head, tail)
    return total


def ancestry(parents):
    prop_count = parents.shape[1]
    indices = jnp.arange(prop_count, dtype=jnp.int32)
    linked = (parents[:, :, None] == indices[None, None, :]).astype(jnp.float32)
    linked = linked + (indices[:, None] == indices[None, :]).astype(jnp.float32)[None]
    for repeat in range(prop_count.bit_length()):
        linked = jnp.minimum(
            jnp.einsum("bij,bjk->bik", linked, linked, precision=lax.Precision.HIGHEST), 1.0
        )
    return linked


def merge_pair(first_part, second_part):
    highest = jnp.maximum(first_part[0], second_part[0])
    scale_first = jnp.exp(first_part[0] - highest)
    scale_second = jnp.exp(second_part[0] - highest)
    seq_count, prop_count, head_count = highest.shape
    outer_first = (
        first_part[2].reshape(seq_count, prop_count, head_count, -1) * scale_first[..., None]
    )
    outer_second = (
        second_part[2].reshape(seq_count, prop_count, head_count, -1) * scale_second[..., None]
    )
    joined = (outer_first + outer_second).reshape(seq_count, prop_count, -1)
    return (highest, first_part[1] * scale_first + second_part[1] * scale_second, joined)


def local(
    tokens,
    norm_gain,
    w_query,
    w_key,
    w_value,
    w_forget,
    forget_bias,
    head_gain,
    w_out,
    cache_keys,
    cache_values,
    cache_gates,
    lengths,
    accepted,
    parents,
):
    seq_count, prop_count, model_width = tokens.shape
    span_rows = cache_keys.shape[1]
    head_count = cache_gates.shape[1]
    head_size = cache_keys.shape[2] // head_count
    scale = head_size ** (-0.5)
    start_pos = lax.axis_index("kv") * span_rows
    positions = start_pos + jnp.arange(span_rows, dtype=jnp.int32)
    valid_len = lengths + accepted
    flat_rows = tokens.reshape(seq_count * prop_count, model_width).astype(jnp.float32)
    normed = (
        flat_rows
        * lax.rsqrt(jnp.mean(flat_rows * flat_rows, axis=1, keepdims=True) + EPSILON)
        * norm_gain.astype(jnp.float32)
    ).astype(jnp.bfloat16)
    picked = (positions[None, :] == (valid_len - 1)[:, None]).astype(jnp.float32)
    last_part = jnp.sum(cache_gates * picked[:, None, :], axis=2)
    row_count = w_query.shape[0]
    own_columns = lax.dynamic_slice_in_dim(normed, lax.axis_index("kv") * row_count, row_count, 1)
    query_part = jnp.dot(own_columns, w_query, preferred_element_type=jnp.float32)
    key_part = jnp.dot(own_columns, w_key, preferred_element_type=jnp.float32)
    value_part = jnp.dot(own_columns, w_value, preferred_element_type=jnp.float32)
    gate_part = jnp.dot(own_columns, w_forget, preferred_element_type=jnp.float32)
    query, fresh_keys, fresh_values, gate_pre, last_gate = lax.psum(
        (query_part, key_part, value_part, gate_part, last_part), "kv"
    )
    query = query.astype(jnp.bfloat16).reshape(seq_count, prop_count, head_count, head_size)
    fresh_keys = fresh_keys.astype(jnp.bfloat16).reshape(
        seq_count, prop_count, head_count, head_size
    )
    fresh_values = fresh_values.astype(jnp.bfloat16).reshape(
        seq_count, prop_count, head_count, head_size
    )
    log_gate = jax.nn.log_sigmoid(gate_pre + forget_bias).reshape(seq_count, prop_count, head_count)
    link = ancestry(parents)
    climb = jnp.einsum("bia,bah->bih", link, log_gate, precision=lax.Precision.HIGHEST)
    stored_keys = cache_keys.reshape(seq_count, span_rows, head_count, head_size)
    stored_values = cache_values.reshape(seq_count, span_rows, head_count, head_size)
    scores = (
        jnp.einsum("bphd,bchd->bphc", query, stored_keys, preferred_element_type=jnp.float32)
        * scale
    )
    scores = scores + (last_gate[:, None, :] + climb)[..., None] - cache_gates[:, None]
    seen = (positions[None, :] < valid_len[:, None])[:, None, None, :]
    highest = jnp.max(jnp.where(seen, scores, NEG_LARGE), axis=3)
    weights = jnp.where(seen, jnp.exp(scores - highest[..., None]), 0.0)
    normalizer = jnp.sum(weights, axis=3)
    weighted = jnp.einsum(
        "bphc,bchd->bphd",
        weights.astype(jnp.bfloat16),
        stored_values,
        preferred_element_type=jnp.float32,
    )
    highest, normalizer, weighted = joined_2(
        (highest, normalizer, weighted.reshape(seq_count, prop_count, head_count * head_size)),
        "kv",
        merge_pair,
    )
    near_scores = (
        jnp.einsum("bphd,bahd->bpha", query, fresh_keys, preferred_element_type=jnp.float32) * scale
    )
    near_scores = near_scores + climb[..., None] - jnp.transpose(climb, (0, 2, 1))[:, None]
    linked = (link > 0.5)[:, :, None, :]
    near_high = jnp.max(jnp.where(linked, near_scores, NEG_LARGE), axis=3)
    overall = jnp.maximum(highest, near_high)
    carried = jnp.exp(highest - overall)
    near_weights = jnp.where(linked, jnp.exp(near_scores - overall[..., None]), 0.0)
    normalizer = normalizer * carried + jnp.sum(near_weights, axis=3)
    attended = weighted.reshape(seq_count, prop_count, head_count, head_size) * carried[..., None]
    attended = attended + jnp.einsum(
        "bpha,bahd->bphd",
        near_weights.astype(jnp.bfloat16),
        fresh_values,
        preferred_element_type=jnp.float32,
    )
    attended = attended / normalizer[..., None]
    gain_rows = head_gain.astype(jnp.float32).reshape(head_count, head_size)
    heads_out = (
        (
            attended
            * lax.rsqrt(jnp.mean(attended * attended, axis=3, keepdims=True) + EPSILON)
            * gain_rows
        )
        .astype(jnp.bfloat16)
        .reshape(seq_count * prop_count, head_count * head_size)
    )
    partial_sum = jnp.dot(heads_out, w_out, preferred_element_type=jnp.float32)
    summed = lax.psum_scatter(partial_sum, "tp", scatter_dimension=1, tiled=True)
    mixed = summed.reshape(seq_count, prop_count, -1)
    offsets = positions[None, :, None] - valid_len[:, None, None]
    placed = offsets == jnp.arange(prop_count, dtype=jnp.int32)[None, None, :]
    landed = jnp.any(placed, axis=2)
    placed_low = placed.astype(jnp.bfloat16)
    written_keys = jnp.einsum(
        "bcj,bjx->bcx",
        placed_low,
        fresh_keys.reshape(seq_count, prop_count, -1),
        preferred_element_type=jnp.float32,
    ).astype(jnp.bfloat16)
    written_values = jnp.einsum(
        "bcj,bjx->bcx",
        placed_low,
        fresh_values.reshape(seq_count, prop_count, -1),
        preferred_element_type=jnp.float32,
    ).astype(jnp.bfloat16)
    keys_out = jnp.where(landed[..., None], written_keys, cache_keys)
    values_out = jnp.where(landed[..., None], written_values, cache_values)
    new_gates = last_gate[:, :, None] + jnp.transpose(climb, (0, 2, 1))
    written_gates = jnp.einsum(
        "bcj,bhj->bhc", placed.astype(jnp.float32), new_gates, precision=lax.Precision.HIGHEST
    )
    gates_out = jnp.where(landed[:, None, :], written_gates, cache_gates)
    return (mixed, keys_out, values_out, gates_out)


HIGHEST = lax.Precision.HIGHEST
MESH = pl.DeviceIdType.MESH
LANES = 128
WINDOW = 16
VMEM_ALL = 67043328


def dot_rows(left, right, precision=None):
    return lax.dot_general(
        left,
        right,
        (((1,), (1,)), ((), ())),
        precision=precision,
        preferred_element_type=jnp.float32,
    )


def dot_plain(left, right, precision=None):
    return jnp.dot(left, right, precision=precision, preferred_element_type=jnp.float32)


def exchange_kernel(
    kv_count,
    head_count,
    lengths_ref,
    accepted_ref,
    tokens_hbm,
    gain_hbm,
    wq_hbm,
    wk_hbm,
    wv_hbm,
    wf_hbm,
    bias_hbm,
    head_gain_hbm,
    wo_hbm,
    keys_hbm,
    values_hbm,
    gates_hbm,
    parents_hbm,
    valid_out,
    mixed_out,
    fresh_out,
    fresh_gates_out,
    keys_ref,
    values_ref,
    gates_ref,
    tokens_ref,
    gain_ref,
    wq_ref,
    wk_ref,
    wv_ref,
    wf_ref,
    bias_ref,
    head_gain_ref,
    wo_ref,
    parents_ref,
    q_send,
    q_recv,
    q_all,
    kv_send,
    kv_recv,
    kv_all,
    g_send,
    g_recv,
    g_all,
    w_send,
    w_recv,
    st_send,
    st_recv,
    h_all,
    o_send,
    o_recv,
    gain_wide,
    load_sem,
    send_sem,
    recv_sem,
    pair_sem,
):
    dp, me, tp = lax.axis_index("dp"), lax.axis_index("kv"), lax.axis_index("tp")
    seq_count, prop, _ = tokens_ref.shape
    depth, width = wq_ref.shape
    span = keys_ref.shape[1]
    head_size = width // head_count
    scale = head_size ** (-0.5)
    rows_all = head_count * prop
    half = wo_ref.shape[1] // 2
    offsets = range(1, kv_count)

    sources = (
        (tokens_hbm, tokens_ref),
        (gain_hbm, gain_ref),
        (wq_hbm, wq_ref),
        (wk_hbm, wk_ref),
        (wv_hbm, wv_ref),
        (wf_hbm, wf_ref),
        (gates_hbm, gates_ref),
        (keys_hbm, keys_ref),
        (values_hbm, values_ref),
        (parents_hbm, parents_ref),
        (bias_hbm, bias_ref),
        (head_gain_hbm, head_gain_ref),
        (wo_hbm, wo_ref),
    )
    loads = {}
    for at, (source, target) in enumerate(sources):
        copy = pltpu.make_async_copy(source, target, load_sem.at[at])
        copy.start()
        loads[id(target)] = copy

    def loaded(*refs):
        for ref in refs:
            loads[id(ref)].wait()

    barrier = pltpu.get_barrier_semaphore()
    for offset in offsets:
        pl.semaphore_signal(
            barrier,
            inc=1,
            device_id=(dp, lax.rem(me + offset, kv_count), tp),
            device_id_type=MESH,
        )
    pl.semaphore_signal(barrier, inc=1, device_id=(dp, me, 1 - tp), device_id_type=MESH)

    started = []

    def send(kind, offset, source, target):
        copy = pltpu.make_async_remote_copy(
            src_ref=source,
            dst_ref=target,
            send_sem=send_sem.at[kind, offset],
            recv_sem=recv_sem.at[kind, offset],
            device_id=(dp, lax.rem(me + offset, kv_count), tp),
            device_id_type=MESH,
        )
        copy.start()
        started.append(copy)
        return copy

    loaded(tokens_ref, gain_ref)
    flat = jnp.concatenate([tokens_ref[s].astype(jnp.float32) for s in range(seq_count)], 0)
    inverse = lax.rsqrt(jnp.mean(flat * flat, axis=1, keepdims=True) + EPSILON)
    start = pl.multiple_of(me * depth, depth)
    own = jnp.concatenate(
        [tokens_ref[s, :, pl.ds(start, depth)].astype(jnp.float32) for s in range(seq_count)], 0
    )
    gain_wide[...] = gain_ref[...].astype(jnp.float32)
    gain_rows = depth // LANES
    own_gain = jnp.concatenate(
        [gain_wide[pl.ds(me * gain_rows + at, 1), :] for at in range(gain_rows)], 1
    )
    normed = (own * inverse * own_gain).astype(jnp.bfloat16)
    loaded(wq_ref)
    q_part = dot_plain(normed, wq_ref[...])
    for s in range(seq_count):
        q_send[s] = q_part[s * prop : (s + 1) * prop]
    pl.semaphore_wait(barrier, kv_count)
    q_copies = [
        send(0, offset, q_send.at[lax.rem(me + offset, kv_count)], q_recv.at[offset])
        for offset in offsets
    ]

    loaded(wk_ref, wv_ref, wf_ref, gates_ref)
    k_part = dot_plain(normed, wk_ref[...])
    for s in range(seq_count):
        kv_send[s, 0] = k_part[s * prop : (s + 1) * prop].astype(jnp.bfloat16)
    v_part = dot_plain(normed, wv_ref[...])
    f_part = dot_rows(wf_ref[...], normed)
    lane_pos = lax.broadcasted_iota(jnp.int32, (head_count, span), 1) + me * span
    for s in range(seq_count):
        valid_out[s] = jnp.full((8, LANES), lengths_ref[s] + accepted_ref[s], jnp.int32)
        rows = slice(s * prop, (s + 1) * prop)
        kv_send[s, 1] = v_part[rows].astype(jnp.bfloat16)
        valid = lengths_ref[s] + accepted_ref[s]
        picked = jnp.where(lane_pos == valid - 1, gates_ref[s], 0.0)
        last = jnp.sum(picked, axis=1, keepdims=True)
        g_send[s] = jnp.broadcast_to(last, (head_count, LANES))
        g_send[s, :, :prop] = f_part[:, rows]

    loaded(parents_ref)
    parent_row = parents_ref[pl.ds(me, 1), :]
    up = lax.broadcasted_iota(jnp.int32, (prop, prop), 0)
    down = lax.broadcasted_iota(jnp.int32, (prop, prop), 1)
    eye = (up == down).astype(jnp.bfloat16)
    linked = jnp.where((up == parent_row) | (up == down), 1.0, 0.0)
    for repeat in range(prop.bit_length()):
        low = linked.astype(jnp.bfloat16)
        linked = jnp.minimum(dot_plain(low, low), 1.0)
    link = dot_rows(eye, linked.astype(jnp.bfloat16))

    total = q_send[me]
    for copy, offset in zip(q_copies, offsets):
        copy.wait_recv()
        total = total + q_recv[offset]
    q_all[me] = total.astype(jnp.bfloat16)
    qa_copies = {offset: send(1, offset, q_all.at[me], q_all.at[me]) for offset in offsets}
    kv_copies = []
    for offset in offsets:
        there = lax.rem(me + offset, kv_count)
        kv_copies.append(send(2, offset, kv_send.at[there, 0], kv_recv.at[offset, 0]))
        kv_copies.append(send(9, offset, kv_send.at[there, 1], kv_recv.at[offset, 1]))
        kv_copies.append(send(3, offset, g_send.at[there], g_recv.at[offset]))

    shape = (head_count, prop, width)
    head_mask = (
        lax.broadcasted_iota(jnp.int32, shape, 2) // head_size
        == lax.broadcasted_iota(jnp.int32, shape, 0)
    )
    small = (head_count, prop, LANES)
    small_lane = lax.broadcasted_iota(jnp.int32, small, 2)
    small_prop = lax.broadcasted_iota(jnp.int32, small, 1)

    def spread(query):
        wide = jnp.broadcast_to(query.astype(jnp.float32)[None], shape)
        return jnp.where(head_mask, wide, 0.0).reshape(rows_all, width).astype(jnp.bfloat16)

    def fold(wide):
        return jnp.sum(jnp.where(head_mask, wide.reshape(shape), 0.0), axis=0)

    def expand(column):
        return fold(jnp.broadcast_to(column, (rows_all, width)))

    def column_of(compact, first_lane):
        wide = jnp.broadcast_to(compact[:, None, :], small)
        taken = jnp.where(small_lane == small_prop + first_lane, wide, 0.0)
        return jnp.sum(taken.reshape(rows_all, LANES), axis=1, keepdims=True)

    score_pos = lax.broadcasted_iota(jnp.int32, (rows_all, span), 1) + me * span

    def attend(s):
        valid = lengths_ref[s] + accepted_ref[s]
        scores = dot_rows(spread(q_all[s]), keys_ref[s]) * scale
        gates = jnp.broadcast_to(gates_ref[s][:, None, :], (head_count, prop, span))
        scores = scores - gates.reshape(rows_all, span)
        seen = score_pos < valid
        highest = jnp.max(jnp.where(seen, scores, NEG_LARGE), axis=1, keepdims=True)
        weights = jnp.where(seen, jnp.exp(scores - highest), 0.0)
        normalizer = jnp.sum(weights, axis=1, keepdims=True)
        w_send[s] = fold(dot_plain(weights.astype(jnp.bfloat16), values_ref[s])).astype(
            jnp.bfloat16
        )
        both = jnp.where(
            small_lane == small_prop,
            highest.reshape(head_count, prop, 1),
            jnp.where(
                small_lane == small_prop + prop,
                normalizer.reshape(head_count, prop, 1),
                0.0,
            ),
        )
        st_send[s] = jnp.sum(both, axis=1)

    loaded(keys_ref, values_ref)
    attend(me)
    w_copies = {}
    for offset in offsets:
        qa_copies[offset].wait_recv()
        back = kv_count - offset
        there = lax.rem(me + back, kv_count)
        attend(there)
        w_copies[back] = (
            send(4, back, w_send.at[there], w_recv.at[back]),
            send(5, back, st_send.at[there], st_recv.at[back]),
        )

    for copy in kv_copies:
        copy.wait_recv()
    fresh_k = kv_send[me, 0].astype(jnp.float32)
    fresh_v = kv_send[me, 1].astype(jnp.float32)
    gate_sum = g_send[me]
    for offset in offsets:
        fresh_k = fresh_k + kv_recv[offset, 0].astype(jnp.float32)
        fresh_v = fresh_v + kv_recv[offset, 1].astype(jnp.float32)
        gate_sum = gate_sum + g_recv[offset]
    fresh_k = fresh_k.astype(jnp.bfloat16)
    fresh_v = fresh_v.astype(jnp.bfloat16)
    kv_all[me, 0] = fresh_k
    kv_all[me, 1] = fresh_v
    loaded(bias_ref)
    square = (head_count, head_count)
    on_diagonal = lax.broadcasted_iota(jnp.int32, square, 0) == lax.broadcasted_iota(
        jnp.int32, square, 1
    )
    bias = jnp.sum(
        jnp.where(on_diagonal, jnp.broadcast_to(bias_ref[...], square), 0.0), axis=1, keepdims=True
    )
    gate_pre = gate_sum[:, :prop] + bias
    log_gate = -(jnp.maximum(-gate_pre, 0.0) + jnp.log1p(jnp.exp(-jnp.abs(gate_pre))))
    climb_rows = dot_plain(log_gate, linked, HIGHEST)
    g_all[me] = jnp.zeros((head_count, LANES), jnp.float32)
    g_all[me, :, :prop] = gate_sum[:, prop : prop + 1] + climb_rows
    climb_wide = jnp.broadcast_to(climb_rows[:, None, :], (head_count, prop, prop))
    climb_col = jnp.sum(
        jnp.where((up == down)[None], climb_wide, 0.0).reshape(rows_all, prop),
        axis=1,
        keepdims=True,
    )
    near_shape = (head_count, prop, prop)
    near = dot_rows(spread(q_all[me]), fresh_k) * scale + climb_col
    near = near - climb_wide.reshape(rows_all, prop)
    near_link = jnp.broadcast_to(link[None], near_shape).reshape(rows_all, prop) > 0.5
    near_high = jnp.max(jnp.where(near_link, near, NEG_LARGE), axis=1, keepdims=True)
    near_weights = jnp.where(near_link, jnp.exp(near - near_high), 0.0)
    near_sum = jnp.sum(near_weights, axis=1, keepdims=True)
    near_wide = dot_plain(near_weights.astype(jnp.bfloat16), fresh_v)
    last_col = jnp.broadcast_to(
        gate_sum[:, prop : prop + 1][:, None, :], (head_count, prop, 1)
    ).reshape(rows_all, 1)
    shift = last_col + climb_col

    fresh_copies = [send(7, offset, kv_all.at[me, 0], kv_all.at[me, 0]) for offset in offsets]

    loaded(head_gain_ref)
    head_gain = head_gain_ref[...].astype(jnp.float32)
    for pair in w_copies.values():
        for copy in pair:
            copy.wait_recv()
    stats = [st_send[me]] + [st_recv[offset] for offset in offsets]
    parts = [w_send[me]] + [w_recv[offset] for offset in offsets]
    highs = [column_of(stat, 0) + shift for stat in stats]
    sums = [column_of(stat, prop) for stat in stats]
    overall = near_high
    for high in highs:
        overall = jnp.maximum(overall, high)
    near_factor = jnp.exp(near_high - overall)
    factors = [jnp.exp(high - overall) for high in highs]
    normalizer = near_sum * near_factor
    for factor, part in zip(factors, sums):
        normalizer = normalizer + factor * part
    attended = fold(near_wide * (near_factor / normalizer))
    for factor, part in zip(factors, parts):
        attended = attended + expand(factor / normalizer) * part.astype(jnp.float32)
    squares = jnp.where(head_mask, jnp.broadcast_to((attended * attended)[None], shape), 0.0)
    square_col = jnp.sum(squares.reshape(rows_all, width), axis=1, keepdims=True)
    rooted = lax.rsqrt(square_col * (1.0 / head_size) + EPSILON)
    head_out = attended * expand(rooted) * jnp.concatenate(
        [head_gain[at : at + 1] for at in range(width // LANES)], 1
    )
    h_all[me] = head_out.astype(jnp.bfloat16)
    h_copies = [send(6, offset, h_all.at[me], h_all.at[me]) for offset in offsets]
    for offset in offsets:
        fresh_copies.append(send(10, offset, kv_all.at[me, 1], kv_all.at[me, 1]))
        fresh_copies.append(send(8, offset, g_all.at[me], g_all.at[me]))

    loaded(wo_ref)
    for copy in h_copies:
        copy.wait_recv()
    heads = jnp.concatenate(
        [h_all[s].astype(jnp.float32) for s in range(seq_count)], 0
    ).astype(jnp.bfloat16)
    there = pl.multiple_of((1 - tp) * half, half)
    here = pl.multiple_of(tp * half, half)
    o_send[...] = dot_plain(heads, wo_ref[:, pl.ds(there, half)])
    pair = pltpu.make_async_remote_copy(
        src_ref=o_send,
        dst_ref=o_recv,
        send_sem=pair_sem.at[0],
        recv_sem=pair_sem.at[1],
        device_id=(dp, me, 1 - tp),
        device_id_type=MESH,
    )
    pair.start()
    own_sum = dot_plain(heads, wo_ref[:, pl.ds(here, half)])
    pair.wait()
    own_sum = own_sum + o_recv[...]
    for s in range(seq_count):
        mixed_out[s] = own_sum[s * prop : (s + 1) * prop]
    for copy in fresh_copies:
        copy.wait_recv()
    fresh_out[...] = kv_all[...]
    fresh_gates_out[...] = g_all[...]
    for copy in started:
        copy.wait_send()


def write_kernel(
    valid_ref,
    mixed_ref,
    fresh_ref,
    fresh_gates_ref,
    keys_ref,
    values_ref,
    gates_ref,
    mixed_out,
    keys_out,
    values_out,
    gates_out,
    window_ref,
    new_gates_ref,
    bulk_sem,
    write_sem,
):
    seq_count, span, width = keys_ref.shape
    prop = fresh_ref.shape[2]
    head_count = gates_ref.shape[1]
    rows = window_ref.shape[2]
    caches = ((keys_ref, keys_out), (values_ref, values_out))
    bulk = [
        pltpu.make_async_copy(source, out, bulk_sem.at[at])
        for at, (source, out) in enumerate(caches + ((mixed_ref, mixed_out),))
    ]
    for copy in bulk:
        copy.start()
    starts = []
    for s in range(seq_count):
        valid = jnp.max(valid_ref[s])
        first = valid - lax.axis_index("kv") * span
        window = jnp.clip(first // WINDOW * WINDOW, 0, span - rows)
        window = pl.multiple_of(window, WINDOW)
        starts.append(window)
        over = lax.broadcasted_iota(jnp.int32, (prop, span), 1) - first
        spot = (over == lax.broadcasted_iota(jnp.int32, (prop, span), 0)).astype(jnp.float32)
        new_gates = dot_plain(fresh_gates_ref[s][:, :prop], spot, HIGHEST)
        lane = lax.broadcasted_iota(jnp.int32, (head_count, span), 1) - first
        new_gates_ref[s] = jnp.where((lane >= 0) & (lane < prop), new_gates, gates_ref[s])
        down = lax.broadcasted_iota(jnp.int32, (rows, prop), 0) + (window - first)
        placed = (down == lax.broadcasted_iota(jnp.int32, (rows, prop), 1)).astype(jnp.bfloat16)
        row = lax.broadcasted_iota(jnp.int32, (rows, width), 0) + (window - first)
        landed = (row >= 0) & (row < prop)
        for at, (source, _) in enumerate(caches):
            written = dot_plain(placed, fresh_ref[s, at])
            old = source[s, pl.ds(window, rows), :].astype(jnp.float32)
            window_ref[at, s] = jnp.where(landed, written, old).astype(jnp.bfloat16)
    writes = [pltpu.make_async_copy(new_gates_ref, gates_out, write_sem.at[2, 0])]
    writes[0].start()
    for at, (_, out) in enumerate(caches):
        bulk[at].wait()
        for s in range(seq_count):
            writes.append(
                pltpu.make_async_copy(
                    window_ref.at[at, s],
                    out.at[s, pl.ds(starts[s], rows), :],
                    write_sem.at[at, s],
                )
            )
            writes[-1].start()
    bulk[2].wait()
    for copy in writes:
        copy.wait()


def fused(
    kv_count,
    tokens,
    norm_gain,
    w_query,
    w_key,
    w_value,
    w_forget,
    forget_bias,
    head_gain,
    w_out,
    cache_keys,
    cache_values,
    cache_gates,
    lengths,
    accepted,
    parents,
):
    seq_count, prop, _ = tokens.shape
    span, width = cache_keys.shape[1:]
    head_count = cache_gates.shape[1]
    half = w_out.shape[1] // 2
    gain = norm_gain.reshape(-1, LANES)
    w_forget = w_forget.T
    bias = forget_bias.reshape(1, -1)
    head_gain = head_gain.reshape(-1, LANES)
    low, high = jnp.bfloat16, jnp.float32
    large = (
        tokens, gain, w_query, w_key, w_value, w_forget, bias, head_gain, w_out,
        cache_keys, cache_values, cache_gates, parents,
    )
    vmem = pltpu.VMEM
    scratch = [vmem(value.shape, value.dtype) for value in large[:9] + large[12:]]
    block = (seq_count, prop, width)
    pair = (seq_count, 2, prop, width)
    scratch += [
        vmem(block, high),
        vmem(block, high),
        vmem(block, low),
        vmem(pair, low),
        vmem(pair, low),
        vmem(pair, low),
        vmem((seq_count, head_count, LANES), high),
        vmem((seq_count, head_count, LANES), high),
        vmem((seq_count, head_count, LANES), high),
        vmem(block, low),
        vmem(block, low),
        vmem((seq_count, head_count, LANES), high),
        vmem((seq_count, head_count, LANES), high),
        vmem(block, low),
        vmem((seq_count * prop, half), high),
        vmem((seq_count * prop, half), high),
        vmem(gain.shape, high),
        pltpu.SemaphoreType.DMA((len(large),)),
        pltpu.SemaphoreType.DMA((11, kv_count)),
        pltpu.SemaphoreType.DMA((11, kv_count)),
        pltpu.SemaphoreType.DMA((2,)),
    ]
    kept = seq_count * (
        prop * half * 4
        + 2 * (prop + span) * width * 2
        + head_count * (LANES + span) * 4
        + 8 * LANES * 4
    )
    smem = pl.BlockSpec(memory_space=pltpu.SMEM)
    held_parts = pl.pallas_call(
        functools.partial(exchange_kernel, kv_count, head_count),
        out_shape=(
            pltpu.VMEM((seq_count, 8, LANES), jnp.int32),
            pltpu.VMEM((seq_count, prop, half), high),
            pltpu.VMEM(pair, low),
            pltpu.VMEM((seq_count, head_count, LANES), high),
            pltpu.VMEM(cache_keys.shape, low),
            pltpu.VMEM(cache_values.shape, low),
            pltpu.VMEM(cache_gates.shape, high),
        ),
        in_specs=[smem, smem] + [pl.BlockSpec(memory_space=pltpu.HBM)] * len(large),
        out_specs=(pl.BlockSpec(memory_space=pltpu.VMEM),) * 7,
        scratch_shapes=scratch,
        compiler_params=pltpu.CompilerParams(
            collective_id=0, has_side_effects=True, vmem_limit_bytes=VMEM_ALL - kept
        ),
        name="exchange",
    )(lengths, accepted, *large)

    held = pl.BlockSpec(memory_space=pltpu.VMEM)
    rows = -(-(prop + WINDOW - 1) // WINDOW) * WINDOW
    far = pl.BlockSpec(memory_space=pltpu.HBM)
    return pl.pallas_call(
        write_kernel,
        out_shape=(
            jax.ShapeDtypeStruct((seq_count, prop, half), high),
            jax.ShapeDtypeStruct(cache_keys.shape, low),
            jax.ShapeDtypeStruct(cache_values.shape, low),
            jax.ShapeDtypeStruct(cache_gates.shape, high),
        ),
        in_specs=[held] * 7,
        out_specs=(far,) * 4,
        scratch_shapes=[
            vmem((2, seq_count, rows, width), low),
            vmem(cache_gates.shape, high),
            pltpu.SemaphoreType.DMA((3,)),
            pltpu.SemaphoreType.DMA((3, seq_count)),
        ],
        compiler_params=pltpu.CompilerParams(vmem_limit_bytes=8 * 1024 * 1024),
        name="write",
    )(*held_parts)


def span_fits(*rest):
    depth, width = rest[1].shape
    span = rest[8].shape[1]
    return span >= 4 * WINDOW and span % WINDOW == span % LANES == depth % LANES == width % LANES == 0


def device_step(kv_count, tp_count, tokens, *rest):
    seq_count, prop, _ = tokens.shape
    head_count = rest[10].shape[1]
    fits = seq_count == kv_count and tp_count == 2 and prop % 8 == 0 and 2 * prop <= LANES
    if fits and kv_count > 1 and head_count % 8 == 0 and span_fits(*rest):
        return fused(kv_count, tokens, *rest)
    return local(tokens, *rest)


def solution(mesh):
    placed = (
        P("dp", None, None),
        P(),
        P("kv", "tp"),
        P("kv", "tp"),
        P("kv", "tp"),
        P("kv", "tp"),
        P("tp"),
        P("tp"),
        P("tp", "kv"),
        P("dp", "kv", "tp"),
        P("dp", "kv", "tp"),
        P("dp", "tp", "kv"),
        P("dp"),
        P("dp"),
        P("dp", None),
    )
    return jax.shard_map(
        functools.partial(device_step, mesh.shape["kv"], mesh.shape["tp"]),
        mesh=mesh,
        in_specs=placed,
        out_specs=(
            P("dp", None, ("kv", "tp")),
            P("dp", "kv", "tp"),
            P("dp", "kv", "tp"),
            P("dp", "tp", "kv"),
        ),
        check_vma=False,
    )
```
